32 devices in a mesh: fs: 8 (over z, x), tp: 4 (over y, core).
Axes of the slice: x: 2, y: 2, z: 4, core: 2. Of those that a mesh axis runs over, the one named last changes fastest.
Arguments:
- inputs: bfloat16 [3072, 2048], P('fs'), may hold values from -6 to 6
- queries: bfloat16 [3072, 2048], P('fs', 'tp'), may hold values from -6 to 6
- keys: bfloat16 [3072, 2048], P('fs', 'tp'), may hold values from -6 to 6
- values: bfloat16 [3072, 2048], P('fs', 'tp'), may hold values from -6 to 6
- head_cot: bfloat16 [3072, 2048], P('fs', 'tp'), may hold values from -6 to 6
- mixing: float32 [16], P('tp'), may hold values from 0.3 to 0.8
- head_gain: float32 [128], replicated, may hold values from 0.1 to 1.9
- factors: bfloat16 [2048, 2, 256], P('fs'), may hold values from -0.375 to 0.375
- moments: float32 [256, 2, 2048], P('fs', None, 'tp'), may hold values from -6 to 6
- weights: float32 [2048, 2, 2048], P('fs', None, 'tp'), may hold values from -6 to 6
Outputs:
- step: float32 [2048, 2, 2048], P('fs', None, 'tp')
- new_moments: float32 [256, 2, 2048], P('fs', None, 'tp')
- copies: bfloat16 [2048, 2, 2048], P(None, None, 'tp')
The draws below stay inside these ranges and needn't reach their ends.
All inputs are finite; a program needn't handle non-finite values.
Results may differ from the reference program's by a relative error of at most 0.007.
Values may be sent and summed in bfloat16 or wider, within the bound.
A program may use at most 64 MiB of HBM per device.

```python
import jax
import jax.numpy as jnp
from jax import lax

D = 2048
HEADS = 16
HEAD_DIM = 64
RANK = 256
TOK_DEV = 384
HV = 2048
TOKENS = 3072


def pair_draw(key):
    shape = (TOKENS, HV)
    first_key, second_key = jax.random.split(jax.random.fold_in(key, 17), 2)
    query_vals = jnp.clip(jax.random.normal(first_key, shape, jnp.float32) * 1.3, -6.0, 6.0)
    key_vals = jnp.clip(jax.random.normal(second_key, shape, jnp.float32) * 1.3, -6.0, 6.0)
    return (query_vals, key_vals)


def draw_queries(key, part):
    return pair_draw(key)[0].astype(jnp.bfloat16)


def draw_keys(key, part):
    return pair_draw(key)[1].astype(jnp.bfloat16)


def steps_of(key, shape, cuts, low, largest):
    gain = 1.0
    for position, shards_of in cuts:
        heights = jax.random.uniform(jax.random.fold_in(jax.random.fold_in(key, 6), position), (shards_of,), jnp.float32, low / len(cuts), largest / len(cuts))
        gain = gain * jnp.repeat(jnp.exp(heights), shape[position] // shards_of).reshape((-1,) + (1,) * (len(shape) - 1 - position))
    return gain


def bell_draw(stream_key, shape, deviation, reach, cuts=(), kind=jnp.bfloat16):
    result = deviation * jax.random.normal(stream_key, shape, jnp.float32)
    if cuts:
        result = result * steps_of(stream_key, shape, cuts, -0.22, 0.18)
    return jnp.clip(result, -reach, reach).astype(kind)


def setup_inputs(seed: int = 0) -> dict:
    splits = jax.random.split(jax.random.key(seed), 11)
    return {
        "inputs": bell_draw(splits[0], (TOKENS, D), 1.0, 6.0, ((0, 8),)),
        "queries": draw_queries(jax.random.fold_in(splits[10], 71), 0),
        "keys": draw_keys(jax.random.fold_in(splits[10], 71), 0),
        "values": bell_draw(splits[3], (TOKENS, HV), 1.0, 6.0, ((0, 8), (1, 4))),
        "head_cot": bell_draw(splits[4], (TOKENS, HV), 1.0, 6.0, ((0, 8), (1, 4))),
        "mixing": jnp.clip(0.3 + 0.5 * jax.random.uniform(splits[5], (HEADS,), jnp.float32) ** steps_of(splits[5], (HEADS,), ((0, 4),), -0.2, 0.2), 0.3, 0.8),
        "head_gain": jnp.clip(1.0 + 0.18 * jax.random.normal(splits[6], (2 * HEAD_DIM,), jnp.float32), 0.1, 1.9),
        "factors": bell_draw(splits[7], (D, 2, RANK), RANK ** -0.5, 0.375, ((0, 8),)),
        "moments": bell_draw(splits[8], (RANK, 2, HV), 1.0, 6.0, ((0, 8), (2, 4)), jnp.float32),
        "weights": bell_draw(splits[9], (D, 2, HV), 1.0, 6.0, ((0, 8), (2, 4)), jnp.float32),
    }


EPS = 0.05
BETA = 0.9
RATE_BASE = 0.5

def softmax_rows(scores):
    top = lax.optimization_barrier(jnp.max(scores, axis=-1, keepdims=True))
    expo = jnp.exp(scores - top)
    return expo / lax.optimization_barrier(jnp.sum(expo, axis=-1, keepdims=True))

def head_grads(query, key_rows, value, upstream, weight_mix, head_gain):
    length = query.shape[0]
    head_dim = query.shape[2]
    factor = head_dim ** (-0.5)
    places = jnp.arange(length)
    causal = places[None, :] <= places[:, None]

    def probs(which):
        scores = jnp.dot(query[:, which], key_rows[:, which].T, preferred_element_type=jnp.float32) * factor
        return softmax_rows(jnp.where(causal, scores, -jnp.inf))
    first = probs(0)
    second = probs(1)
    mixed = (first - weight_mix * second).astype(jnp.bfloat16)
    output = jnp.dot(mixed, value, preferred_element_type=jnp.float32)
    inverse = lax.rsqrt(lax.optimization_barrier(jnp.mean(output * output, axis=-1, keepdims=True)) + EPS)
    scaled = head_gain * upstream.astype(jnp.float32)
    d_out = inverse * scaled - output * inverse ** 3 * lax.optimization_barrier(jnp.mean(output * scaled, axis=-1, keepdims=True))
    d_out = d_out.astype(jnp.bfloat16)
    d_value = jnp.dot(mixed.T, d_out, preferred_element_type=jnp.float32).astype(jnp.bfloat16)
    d_mix = jnp.dot(d_out, value.T, preferred_element_type=jnp.float32)
    d_first = (first * (d_mix - lax.optimization_barrier(jnp.sum(first * d_mix, axis=-1, keepdims=True)))).astype(jnp.bfloat16)
    d_second = (-weight_mix * second * (d_mix - lax.optimization_barrier(jnp.sum(second * d_mix, axis=-1, keepdims=True)))).astype(jnp.bfloat16)
    q_first = (jnp.dot(d_first, key_rows[:, 0], preferred_element_type=jnp.float32) * factor).astype(jnp.bfloat16)
    q_second = (jnp.dot(d_second, key_rows[:, 1], preferred_element_type=jnp.float32) * factor).astype(jnp.bfloat16)
    return (jnp.stack([q_first, q_second], axis=1).reshape(length, 2 * head_dim), d_value)

def reference(inputs, queries, keys, values, head_cot, mixing, head_gain, factors, moments, weights):
    sequences = TOKENS // TOK_DEV
    query_all = queries.reshape(sequences, TOK_DEV, HEADS, 2, HEAD_DIM)
    key_all = keys.reshape(sequences, TOK_DEV, HEADS, 2, HEAD_DIM)
    value_all = values.reshape(sequences, TOK_DEV, HEADS, 2 * HEAD_DIM)
    upstream_all = head_cot.reshape(sequences, TOK_DEV, HEADS, 2 * HEAD_DIM)
    per_head = jax.vmap(head_grads, in_axes=(1, 1, 1, 1, 0, None))

    def one_sequence(pieces):
        return per_head(pieces[0], pieces[1], pieces[2], pieces[3], mixing, head_gain)
    d_query, d_value = lax.map(one_sequence, (query_all, key_all, value_all, upstream_all))
    d_query = d_query.transpose(0, 2, 1, 3).reshape(TOKENS, HV)
    d_value = d_value.transpose(0, 2, 1, 3).reshape(TOKENS, HV)
    cotangents = jnp.stack([d_query, d_value], axis=1).reshape(TOKENS, 2 * HV)
    grads = jnp.dot(inputs.T, cotangents, preferred_element_type=jnp.float32).reshape(D, 2, HV)
    grads = grads * TOKENS ** (-0.5)
    factor_wide = factors.astype(jnp.float32)
    projected = jnp.einsum('dkr,dke->rke', factor_wide, grads, precision=lax.Precision.HIGHEST)
    new_moments = BETA * moments + projected
    totals = lax.optimization_barrier(jnp.sum(new_moments * new_moments, axis=(0, 2)))
    rate = RATE_BASE / jnp.sqrt(1.0 + totals / (RANK * HV))
    step = jnp.einsum('dkr,rke->dke', factor_wide, new_moments, precision=lax.Precision.HIGHEST) * rate[None, :, None]
    copies = (weights - step).astype(jnp.bfloat16)
    return (step, new_moments, copies)
```

```python
import functools

import jax
import jax.numpy as jnp
from jax import lax
from jax.experimental import pallas as pl
from jax.experimental.pallas import tpu as pltpu
from jax.sharding import PartitionSpec as P

EPS = 0.05
BETA = 0.9
RATE_BASE = 0.5
MESH = pl.DeviceIdType.MESH
LANES = 128
CHUNKS = 8
WIDE = 1
DEPTH = 2


def split(ref, t, tiles, count):
    return ref[pl.ds(t % tiles * 2 + t // tiles, count, stride=2 * tiles), :]


def head_step(head, q_ref, k_ref, v_ref, c_ref, mix_ref, gain_ref, dq_ref, dv_ref):
    length = q_ref.shape[0]
    width = gain_ref.shape[1]
    half = width // 2
    factor = half ** (-0.5)
    cols = slice(head * width, (head + 1) * width)
    query, key, value = q_ref[:, cols], k_ref[:, cols], v_ref[:, cols]
    lane = lax.broadcasted_iota(jnp.int32, (length, width), 1)
    zero = jnp.zeros_like(key)
    key0 = jnp.where(lane < half, key, zero)
    key1 = jnp.where(lane < half, zero, key)
    row = lax.broadcasted_iota(jnp.int32, (length, length), 0)
    col = lax.broadcasted_iota(jnp.int32, (length, length), 1)
    causal = col <= row
    mix = mix_ref[head]
    nt = (((1,), (1,)), ((), ()))
    tn = (((0,), (0,)), ((), ()))

    def probs(rows):
        scores = lax.dot_general(query, rows, nt, preferred_element_type=jnp.float32) * factor
        scores = jnp.where(causal, scores, -jnp.inf)
        expo = jnp.exp(scores - jnp.max(scores, axis=-1, keepdims=True))
        return expo * (1.0 / jnp.sum(expo, axis=-1, keepdims=True))

    first, second = probs(key0), probs(key1)
    mixed = (first - mix * second).astype(jnp.bfloat16)
    output = jnp.dot(mixed, value, preferred_element_type=jnp.float32)
    inverse = lax.rsqrt(jnp.mean(output * output, axis=-1, keepdims=True) + EPS)
    scaled = gain_ref[...] * c_ref[:, cols].astype(jnp.float32)
    d_out = inverse * scaled - output * (inverse * inverse * inverse) * jnp.mean(
        output * scaled, axis=-1, keepdims=True
    )
    d_out = d_out.astype(jnp.bfloat16)
    dv_ref[:, cols] = lax.dot_general(mixed, d_out, tn, preferred_element_type=jnp.float32).astype(jnp.bfloat16)
    d_mix = lax.dot_general(d_out, value, nt, preferred_element_type=jnp.float32)
    d_first = first * (d_mix - jnp.sum(first * d_mix, axis=-1, keepdims=True))
    d_second = -mix * second * (d_mix - jnp.sum(second * d_mix, axis=-1, keepdims=True))
    d_query = jnp.dot(d_first.astype(jnp.bfloat16), key0, preferred_element_type=jnp.float32)
    d_query += jnp.dot(d_second.astype(jnp.bfloat16), key1, preferred_element_type=jnp.float32)
    dq_ref[:, cols] = (d_query * factor).astype(jnp.bfloat16)


class Lists:
    def __init__(self):
        def source(k, order):
            return [(k, True, c) for c in order] + [(k, False, c) for c in range(WIDE)]

        order = list(range(WIDE, CHUNKS)) + list(range(WIDE))
        mirror = lambda entries: [(3 - k, same, c) for k, same, c in entries]
        first = source(0, order)
        inner = source(1, order)
        self.up = {0: first, 1: self.merge(inner, first)}
        far = mirror(self.up[1])
        self.down = {0: [], 1: self.merge(inner, far)}
        self.from_up = {0: self.down[1], 1: far}
        self.from_down = {0: [], 1: first}
        own = lambda q: [(q, True, c) for c in range(CHUNKS)]
        narrow = lambda entries: [e for e in entries if e[1] and e[2] >= WIDE]
        self.cross = {
            0: own(0) + narrow(self.from_up[0]),
            1: own(1) + self.weave(narrow(self.from_down[1]), narrow(self.from_up[1])),
        }
        self.from_cross = {q: [(k, not same, c) for k, same, c in self.cross[q]] for q in (0, 1)}

    @staticmethod
    def merge(own, passed):
        return own + passed

    @staticmethod
    def weave(a, b):
        out = []
        for i in range(max(len(a), len(b))):
            out += a[i : i + 1] + b[i : i + 1]
        return out


class Weights:
    def __init__(self, lists, q):
        self.q = q
        self.out = {"up": list(lists.up[q]), "down": list(lists.down[q]), "cross": list(lists.cross[q])}
        self.into = {
            "cross": list(lists.from_cross[q]), "down": list(lists.from_down[q]), "up": list(lists.from_up[q]),
        }
        self.have = {(q, True, c) for c in range(CHUNKS)}
        self.got = {way: 0 for way in self.into}
        self.put = {way: 0 for way in self.out}
        self.round = 0

    def fill(self, depth, limit=None):
        moves = []
        for way in ("up", "down", "cross"):
            while self.put[way] < min(len(self.out[way]), self.round + depth):
                entry = self.out[way][self.put[way]]
                if entry not in self.have:
                    break
                moves.append(("send", way, entry))
                self.put[way] += 1
        return moves

    def turn(self, lag, depth):
        moves = self.fill(depth)
        self.round += 1
        for way in ("cross", "down", "up"):
            while self.got[way] < min(len(self.into[way]), self.round - lag):
                entry = self.into[way][self.got[way]]
                moves.append(("wait", way, entry))
                self.have.add(entry)
                self.got[way] += 1
                moves += self.fill(depth)
        return moves

    def done(self):
        return all(self.got[w] == len(self.into[w]) for w in self.into) and all(
            self.put[w] == len(self.out[w]) for w in self.out
        )


def kernel(
    n, tp, heads,
    x_hbm, q_hbm, k_hbm, v_hbm, c_hbm, mix_hbm, gain_hbm, f_hbm, mom_hbm, w_hbm,
    wall, low, nm_ref, tot_ref,
    x_ref, q_ref, k_ref, v_ref, c_ref, mix_ref, gain_ref, f_ref, mom_ref, w_ref,
    fall, nmall, fwide, dq, dv, psend, precv, sums,
    l_sem, f_send, f_recv, s_send, s_recv, w_send, w_recv, n_send, n_recv, p_send, p_recv, t_send, t_recv,
):
    me = lax.axis_index("fs")
    mt = lax.axis_index("tp")
    depth = fall.shape[0]
    deep = depth // n
    rank = fall.shape[1] // 2
    rank_here = rank // n
    cols = dq.shape[1]
    tiles_f, tiles_w = rank // LANES, cols // LANES
    per_row = 2 * tiles_w

    local = {}
    for i, (name, src, dst) in enumerate((
        ("f", f_hbm, f_ref), ("w", w_hbm, w_ref), ("gain", gain_hbm, gain_ref), ("mix", mix_hbm, mix_ref),
        ("q", q_hbm, q_ref), ("k", k_hbm, k_ref), ("v", v_hbm, v_ref), ("c", c_hbm, c_ref),
        ("x", x_hbm, x_ref), ("mom", mom_hbm, mom_ref),
    )):
        local[name] = pltpu.make_async_copy(src, dst, l_sem.at[i])
        local[name].start()

    barrier = pltpu.get_barrier_semaphore()
    for hop in range(1, n):
        pl.semaphore_signal(barrier, inc=1, device_id={"fs": (me + hop) % n}, device_id_type=MESH)
    for hop in range(1, tp):
        pl.semaphore_signal(barrier, inc=1, device_id={"tp": (mt + hop) % tp}, device_id_type=MESH)

    local["f"].wait()
    fwide[...] = f_ref[...].astype(jnp.float32)
    here = pl.ds(pl.multiple_of(me * deep, deep), deep)
    for t in range(2 * tiles_f):
        fall[here, t * LANES : (t + 1) * LANES] = split(fwide, t, tiles_f, deep).astype(jnp.bfloat16)
    local["w"].wait()
    wall[pl.ds(pl.multiple_of(me * deep * per_row, 16), deep * per_row), :] = w_ref[...].astype(jnp.bfloat16)
    for name in ("gain", "mix", "q", "k", "v", "c"):
        local[name].wait()

    def head(i):
        head_step(i, q_ref, k_ref, v_ref, c_ref, mix_ref, gain_ref, dq, dv)

    def remote(src, send, recv, axis, target):
        return pltpu.make_async_remote_copy(
            src_ref=src, dst_ref=src, send_sem=send, recv_sem=recv, device_id={axis: target}, device_id_type=MESH
        )

    def project():
        local["x"].wait()
        for m, cot in enumerate((dq, dv)):
            reduced = jnp.dot(
                x_ref[...], fall[:, m * rank : (m + 1) * rank], preferred_element_type=jnp.float32
            ).astype(jnp.bfloat16)
            partial = lax.dot_general(
                reduced, cot[...], (((0,), (0,)), ((), ())), preferred_element_type=jnp.float32
            )
            for j in range(n):
                psend[j, m] = partial[j * rank_here : (j + 1) * rank_here].astype(psend.dtype)

    def p_copy(hop):
        peer = (me + hop) % n
        return pltpu.make_async_remote_copy(
            src_ref=psend.at[peer], dst_ref=precv.at[hop], send_sem=p_send.at[hop], recv_sem=p_recv.at[hop],
            device_id={"fs": peer}, device_id_type=MESH,
        )

    def momentum():
        local["mom"].wait()
        total = psend[me].astype(jnp.float32)
        for hop in range(1, n):
            p_copy(hop).wait_recv()
            total += precv[hop].astype(jnp.float32)
        length = x_ref.shape[0]
        for t in range(2 * tiles_w):
            m, lanes = t // tiles_w, slice(t % tiles_w * LANES, (t % tiles_w + 1) * LANES)
            moments = BETA * split(mom_ref, t, tiles_w, rank_here)
            moments += total[m, :, lanes] * (length * n) ** (-0.5)
            nm_ref[pl.ds(t % tiles_w * 2 + m, rank_here, stride=per_row), :] = moments
            nmall[me, m, :, lanes] = moments.astype(nmall.dtype)

    def t_copy(hop):
        return pltpu.make_async_remote_copy(
            src_ref=sums.at[0], dst_ref=sums.at[hop], send_sem=t_send.at[hop], recv_sem=t_recv.at[hop],
            device_id={"tp": (mt + hop) % tp}, device_id_type=MESH,
        )

    def squares():
        everything = nmall[...].astype(jnp.float32)
        parts = jnp.sum(jnp.sum(everything * everything, axis=0), axis=1)
        sums[0] = jnp.sum(parts, axis=1, keepdims=True) + jnp.zeros((2, LANES), jnp.float32)
        for hop in range(1, tp):
            t_copy(hop).start()

    def totals():
        result = sums[0]
        for hop in range(1, tp):
            t_copy(hop).wait_recv()
            result += sums[hop]
        tot_ref[...] = result

    def lows(start, count):
        for m in range(2):
            block = nmall[:, m].reshape(rank, cols).astype(jnp.bfloat16)
            product = jnp.dot(
                fall[start : start + count, m * rank : (m + 1) * rank], block, preferred_element_type=jnp.float32
            )
            for t in range(tiles_w):
                low[pl.ds(start * per_row + 2 * t + m, count, stride=per_row), :] = (
                    product[:, t * LANES : (t + 1) * LANES]
                )

    def weights(index, chunk, chunks):
        size = deep // chunks * per_row
        return wall.at[pl.ds(pl.multiple_of(index * deep * per_row + chunk * size, 16), size)]

    quarter = 2 * rank // tp
    if n == 8 and tp == 4 and quarter % LANES == 0 and deep % (2 * CHUNKS) == 0:
        place, parity = me // 2, me % 2
        flip = place // 2
        side = jnp.where(flip == 0, place, 3 - place)
        lists = Lists()
        states = [Weights(lists, q) for q in (0, 1)]
        partner = me + 1 - 2 * parity
        far, near = (mt + 2) % tp, mt + 1 - 2 * (mt % 2)

        def index_of(k, same):
            return 2 * (k + flip * (3 - 2 * k)) + (parity if same else 1 - parity)

        def target(q, way):
            return partner if way == "cross" else index_of(q + 1 if way == "up" else q - 1, True)

        ways = {"up": 0, "down": 1, "cross": 2}

        def w_copy(q, way, entry):
            k, same, chunk = entry
            index = index_of(k, same)
            return remote(
                weights(index, chunk, CHUNKS), w_send.at[index, chunk, ways[way]], w_recv.at[index, chunk],
                "fs", target(q, way),
            )

        def run(q, moves):
            for kind, way, entry in moves:
                if kind == "send":
                    w_copy(q, way, entry).start()
                else:
                    w_copy(q, "cross", entry).wait_recv()

        def piece(index, which):
            return fall.at[
                pl.ds(pl.multiple_of(index * deep, deep), deep), pl.ds(pl.multiple_of(which * quarter, quarter), quarter)
            ]

        def others(q):
            return sorted((k for k in range(4) if k != q), key=lambda k: (abs(k - q), k))

        def small(kind, index, way, to):
            if kind == "f":
                return remote(piece(index, mt), f_send.at[index, way], f_recv.at[index], "fs", to)
            return remote(nmall.at[index], n_send.at[index, way], n_recv.at[index], "fs", to)

        def small_begin(kind, q):
            for i, k in enumerate(reversed(others(q))):
                small(kind, me, i, index_of(k, True)).start()
            small(kind, me, 3, partner).start()

        def spread(index, which, to, way):
            return remote(piece(index, which), s_send.at[index, way], s_recv.at[index, way], "tp", to)

        def small_wait(kind, q, k, same):
            index = index_of(k, same)
            small(kind, index, 0, partner).wait_recv()
            if same:
                small(kind, index, 0, partner).start()
            if kind == "f":
                spread(index, mt, far, 0).start()
                spread(index, mt, near, 1).start()

        def pieces(q):
            return [(q, False)] + [(k, True) for k in others(q)] + [(k, False) for k in others(q)]

        def segment(tokens):
            for q in (0, 1):

                @pl.when(side == q)
                def _(q=q):
                    for token in tokens:
                        kind, *rest = token
                        if kind == "w":
                            lag, count = rest
                            for _ in range(count):
                                run(q, states[q].turn(lag, DEPTH))
                        elif kind == "begin":
                            small_begin(rest[0], q)
                        elif kind == "fill":
                            run(q, states[q].fill(rest[0]))
                        elif kind == "small":
                            for i in rest[1]:
                                small_wait(rest[0], q, *pieces(q)[i])
                        elif kind == "all":
                            while not states[q].done():
                                run(q, states[q].turn(*rest, DEPTH))
                        elif kind == "spread":
                            for k, same in pieces(q):
                                index = index_of(k, same)
                                spread(index, far, far, 0).wait_recv()
                                spread(index, far, near, 2).start()
                            for k, same in pieces(q):
                                index = index_of(k, same)
                                spread(index, near, near, 1).wait_recv()
                                spread(index, (near + 2) % tp, near, 2).wait_recv()
                        elif kind == "sent":
                            for way in ways:
                                for entry in states[q].out[way]:
                                    w_copy(q, way, entry).wait_send()
                            for name in ("f", "n"):
                                for way in range(4):
                                    small(name, me, way, partner).wait_send()
                                for k in others(q):
                                    small(name, index_of(k, True), 0, partner).wait_send()
                            for k, same in pieces(q):
                                for way in range(3):
                                    spread(index_of(k, same), mt, near, way).wait_send()

        head(0)
        pl.semaphore_wait(barrier, n - 1 + tp - 1)
        segment([("begin", "f"), ("fill", DEPTH)])
        head(1)
        segment([("small", "f", (0,)), ("w", 4, 1)])
        head(2)
        segment([("small", "f", (1, 2)), ("w", 4, 1)])
        head(3)
        for i in range(4, heads):
            head(i)
        segment([("w", 4, 1), ("small", "f", (3,)), ("w", 4, 2), ("small", "f", (4, 5, 6)), ("w", 4, 1), ("spread",)])
        project()
        for hop in range(1, n):
            p_copy(hop).start()
        segment([("w", 4, 8)])
        momentum()
        segment([
            ("begin", "n"), ("w", 4, 2), ("small", "n", (0, 1, 2)), ("w", 4, 2), ("small", "n", (3,)), ("w", 4, 2),
            ("small", "n", (4, 5, 6)),
        ])
        squares()
        for j in range(n):
            lows(j * deep, deep)
            segment([("w", 4, 1)])
        totals()
        segment([("all", 4)])
        segment([("sent",)])
    else:
        for i in range(heads):
            head(i)
        pl.semaphore_wait(barrier, n - 1 + tp - 1)

        def block(kind, index, hop):
            if kind == "f":
                return remote(
                    fall.at[pl.ds(pl.multiple_of(index * deep, 8), deep)], f_send.at[hop], f_recv.at[index],
                    "fs", (me + hop) % n,
                )
            if kind == "w":
                return remote(weights(index, 0, 1), w_send.at[hop], w_recv.at[index], "fs", (me + hop) % n)
            return remote(nmall.at[index], n_send.at[hop], n_recv.at[index], "fs", (me + hop) % n)

        def each(action):
            def step(hop, carry):
                action(hop)
                return carry

            lax.fori_loop(1, n, step, 0)

        each(lambda hop: block("f", me, hop).start())
        each(lambda hop: block("w", me, hop).start())
        each(lambda hop: block("f", (me + hop) % n, hop).wait_recv())
        project()
        each(lambda hop: p_copy(hop).start())
        momentum()
        each(lambda hop: block("n", me, hop).start())
        each(lambda hop: block("n", (me + hop) % n, hop).wait_recv())
        squares()
        for start in range(0, depth, 256):
            lows(start, min(256, depth - start))
        totals()
        each(lambda hop: block("w", (me + hop) % n, hop).wait_recv())
        for kind in ("f", "w", "n"):
            each(lambda hop, kind=kind: block(kind, me, hop).wait_send())
    for hop in range(1, tp):
        t_copy(hop).wait_send()
    for hop in range(1, n):
        p_copy(hop).wait_send()


def finish(n, entries, wall, low, nm_ref, tot_ref, step_hbm, nm_hbm, copies_hbm, step, copies, sems):
    me = lax.axis_index("fs")
    rows = low.shape[0]
    own = rows // n
    nm_copy = pltpu.make_async_copy(nm_ref, nm_hbm, sems.at[0])
    nm_copy.start()
    rate = RATE_BASE / jnp.sqrt(1.0 + tot_ref[...] / entries)
    count = min(rows // 16, 1024)
    odd = lax.broadcasted_iota(jnp.int32, (count, LANES), 0) % 2 == 1
    rates = jnp.where(odd, rate[1:2], rate[0:1])
    started = [nm_copy]
    for i in range(0, own, min(count, own)):
        size = min(count, own)
        start = pl.multiple_of(me * own + i, 8)
        step[i : i + size, :] = low[pl.ds(start, size), :] * rates[:size]
    started.append(pltpu.make_async_copy(step, step_hbm, sems.at[1]))
    started[-1].start()
    for i in range(rows // count):
        at = slice(i * count, (i + 1) * count)
        copies[at, :] = (wall[at, :].astype(jnp.float32) - low[at, :] * rates).astype(jnp.bfloat16)
        started.append(pltpu.make_async_copy(copies.at[at], copies_hbm.at[at], sems.at[2 + i]))
        started[-1].start()
    for copy in started:
        copy.wait()


def to_rows(array):
    rows, maps, cols = array.shape
    return array.reshape(rows, maps, cols // LANES, LANES).transpose(0, 2, 1, 3).reshape(-1, LANES)


def from_rows(array, rows):
    return (
        array.reshape(rows, -1, 2, LANES).transpose(0, 2, 1, 3).reshape(rows, 2, -1)
    )


def per_device(
    n, tp, inputs, queries, keys, values, head_cot, mixing, head_gain, factors, moments, weights
):
    length, depth = inputs.shape
    heads = mixing.shape[0]
    deep, _, rank = factors.shape
    rank_here, _, cols = moments.shape
    wire = jnp.bfloat16 if rank_here % 16 == 0 else jnp.float32
    per_row = 2 * cols // LANES
    hbm = pl.BlockSpec(memory_space=pltpu.HBM)
    vmem = pl.BlockSpec(memory_space=pltpu.VMEM)
    dma = pltpu.SemaphoreType.DMA
    args = (
        inputs, queries, keys, values, head_cot, mixing, head_gain[None, :],
        to_rows(factors), to_rows(moments), to_rows(weights),
    )
    held = pl.pallas_call(
        functools.partial(kernel, n, tp, heads),
        out_shape=(
            pltpu.VMEM((depth * per_row, LANES), jnp.bfloat16),
            pltpu.VMEM((depth * per_row, LANES), jnp.float32),
            pltpu.VMEM((rank_here * per_row, LANES), jnp.float32),
            pltpu.VMEM((2, LANES), jnp.float32),
        ),
        in_specs=[hbm] * len(args),
        out_specs=(vmem,) * 4,
        scratch_shapes=[
            pltpu.VMEM((length, depth), jnp.bfloat16),
            pltpu.VMEM((length, cols), jnp.bfloat16),
            pltpu.VMEM((length, cols), jnp.bfloat16),
            pltpu.VMEM((length, cols), jnp.bfloat16),
            pltpu.VMEM((length, cols), jnp.bfloat16),
            pltpu.SMEM((heads,), jnp.float32),
            pltpu.VMEM((1, head_gain.shape[0]), jnp.float32),
            pltpu.VMEM((deep * 2 * rank // LANES, LANES), jnp.bfloat16),
            pltpu.VMEM((rank_here * per_row, LANES), jnp.float32),
            pltpu.VMEM((deep * per_row, LANES), jnp.float32),
            pltpu.VMEM((depth, 2 * rank), jnp.bfloat16),
            pltpu.VMEM((n, 2, rank_here, cols), wire),
            pltpu.VMEM((deep * 2 * rank // LANES, LANES), jnp.float32),
            pltpu.VMEM((length, cols), jnp.bfloat16),
            pltpu.VMEM((length, cols), jnp.bfloat16),
            pltpu.VMEM((n, 2, rank_here, cols), wire),
            pltpu.VMEM((n, 2, rank_here, cols), wire),
            pltpu.VMEM((tp, 2, LANES), jnp.float32),
            dma((len(args),)),
            *(
                (
                    dma((n, 4)), dma((n,)), dma((n, 3)), dma((n, 3)),
                    dma((n, CHUNKS, 3)), dma((n, CHUNKS)), dma((n, 4)), dma((n,)),
                )
                if n == 8
                else (dma((n,)), dma((n,)), dma((1,)), dma((1,)), dma((n,)), dma((n,)), dma((n,)), dma((n,)))
            ),
            dma((n,)), dma((n,)),
            dma((tp,)), dma((tp,)),
        ],
        compiler_params=pltpu.CompilerParams(
            collective_id=0, has_side_effects=True, vmem_limit_bytes=36 * 1024 * 1024
        ),
    )(*(pltpu.with_memory_space_constraint(arg, pltpu.HBM) for arg in args))
    out_hbm = pl.BlockSpec(memory_space=pltpu.HBM)
    step, new_moments, copies = pl.pallas_call(
        functools.partial(finish, n, rank * cols * tp),
        out_shape=(
            jax.ShapeDtypeStruct((deep * per_row, LANES), jnp.float32),
            jax.ShapeDtypeStruct((rank_here * per_row, LANES), jnp.float32),
            jax.ShapeDtypeStruct((depth * per_row, LANES), jnp.bfloat16),
        ),
        in_specs=[vmem] * 4,
        out_specs=(out_hbm,) * 3,
        scratch_shapes=[
            pltpu.VMEM((deep * per_row, LANES), jnp.float32),
            pltpu.VMEM((depth * per_row, LANES), jnp.bfloat16),
            dma((18,)),
        ],
        compiler_params=pltpu.CompilerParams(vmem_limit_bytes=16 * 1024 * 1024),
    )(*held)
    return from_rows(step, deep), from_rows(new_moments, rank_here), from_rows(copies, depth)


def solution(mesh):
    placed = (
        P("fs", None),
        P("fs", "tp"),
        P("fs", "tp"),
        P("fs", "tp"),
        P("fs", "tp"),
        P("tp"),
        P(),
        P("fs", None, None),
        P("fs", None, "tp"),
        P("fs", None, "tp"),
    )
    return jax.shard_map(
        functools.partial(per_device, mesh.shape["fs"], mesh.shape["tp"]),
        mesh=mesh,
        in_specs=placed,
        out_specs=(P("fs", None, "tp"), P("fs", None, "tp"), P(None, None, "tp")),
        check_vma=False,
    )
```

```python
import functools

import jax
import jax.numpy as jnp
from jax import lax
from jax.experimental import pallas as pl
from jax.experimental.pallas import tpu as pltpu
from jax.sharding import PartitionSpec as P

EPS = 0.05
BETA = 0.9
RATE_BASE = 0.5
MESH = pl.DeviceIdType.MESH
LANES = 128
CHUNKS = 8
WIDE = 2
DIRECT = ()
SCHEDULE = [
    ("begin", "f"), ("w", 0, 0, 4, 2),
    ("head", 1),
    ("small", "f", (0,)), ("w", 0, 0, 5, 2),
    ("head", 2),
    ("small", "f", (1, 2)), ("w", 0, 0, 10, 2),
    ("head", 3),
    ("small", "f", (3,)), ("w", 0, 0, 10, 8), ("small", "f", (4, 5, 6)), ("spread",),
    ("w", 6, 6, 12, 10),
    ("project",),
    ("px",), ("w", 8, 8, 14, 10), ("w", 9, 8, 15, 10),
    ("pz", (0,)), ("w", 10, 8, 15, 10), ("pz", (1,)), ("w", 11, 8, 15, 11), ("pz", (2,)), ("pz", (3,)),
    ("w", 12, 9, 15, 12), ("w", 13, 10, 16, 13), ("w", 14, 11, 17, 14),
    ("momentum",),
    ("begin", "n"), ("w", 14, 11, 17, 14), ("w", 15, 12, 18, 15), ("w", 16, 13, 19, 16),
    ("small", "n", (0,)), ("small", "n", (1,)), ("w", 17, 14, 20, 16), ("small", "n", (2,)), ("w", 18, 14, 21, 16),
    ("small", "n", (3,)), ("w", 19, 15, 22, 17), ("small", "n", (4,)), ("w", 20, 15, 23, 18), ("small", "n", (5,)),
    ("w", 21, 16, 24, 19),
    ("small", "n", (6,)),
    ("squares",),
]
for j in range(8):
    SCHEDULE += [("lows", j), ("w", 22 + j, 17 + j, 25 + j, 20 + j)]
SCHEDULE += [("totals",), ("all", 30, 25, 3)]


def split(ref, t, tiles, count):
    return ref[pl.ds(t % tiles * 2 + t // tiles, count, stride=2 * tiles), :]


def head_step(head, q_ref, k_ref, v_ref, c_ref, mix_ref, gain_ref, dq_ref, dv_ref):
    length = q_ref.shape[0]
    width = gain_ref.shape[1]
    half = width // 2
    factor = half ** (-0.5)
    cols = slice(head * width, (head + 1) * width)
    query, key, value = q_ref[:, cols], k_ref[:, cols], v_ref[:, cols]
    lane = lax.broadcasted_iota(jnp.int32, (length, width), 1)
    zero = jnp.zeros_like(key)
    key0 = jnp.where(lane < half, key, zero)
    key1 = jnp.where(lane < half, zero, key)
    row = lax.broadcasted_iota(jnp.int32, (length, length), 0)
    col = lax.broadcasted_iota(jnp.int32, (length, length), 1)
    causal = col <= row
    mix = mix_ref[head]
    nt = (((1,), (1,)), ((), ()))
    tn = (((0,), (0,)), ((), ()))

    def probs(rows):
        scores = lax.dot_general(query, rows, nt, preferred_element_type=jnp.float32) * factor
        scores = jnp.where(causal, scores, -jnp.inf)
        expo = jnp.exp(scores - jnp.max(scores, axis=-1, keepdims=True))
        return expo * (1.0 / jnp.sum(expo, axis=-1, keepdims=True))

    first, second = probs(key0), probs(key1)
    mixed = (first - mix * second).astype(jnp.bfloat16)
    output = jnp.dot(mixed, value, preferred_element_type=jnp.float32)
    inverse = lax.rsqrt(jnp.mean(output * output, axis=-1, keepdims=True) + EPS)
    scaled = gain_ref[...] * c_ref[:, cols].astype(jnp.float32)
    d_out = inverse * scaled - output * (inverse * inverse * inverse) * jnp.mean(
        output * scaled, axis=-1, keepdims=True
    )
    d_out = d_out.astype(jnp.bfloat16)
    dv_ref[:, cols] = lax.dot_general(mixed, d_out, tn, preferred_element_type=jnp.float32).astype(jnp.bfloat16)
    d_mix = lax.dot_general(d_out, value, nt, preferred_element_type=jnp.float32)
    d_first = first * (d_mix - jnp.sum(first * d_mix, axis=-1, keepdims=True))
    d_second = -mix * second * (d_mix - jnp.sum(second * d_mix, axis=-1, keepdims=True))
    d_query = jnp.dot(d_first.astype(jnp.bfloat16), key0, preferred_element_type=jnp.float32)
    d_query += jnp.dot(d_second.astype(jnp.bfloat16), key1, preferred_element_type=jnp.float32)
    dq_ref[:, cols] = (d_query * factor).astype(jnp.bfloat16)


class Lists:
    def __init__(self):
        def source(k, order):
            return [(k, True, c) for c in order] + [(k, False, c) for c in range(WIDE)]

        order = list(range(WIDE, CHUNKS)) + list(range(WIDE))
        mirror = lambda entries: [(3 - k, same, c) for k, same, c in entries]
        first = source(0, order)
        inner = source(1, order)
        self.up = {0: first, 1: self.merge(inner, first)}
        far = mirror(self.up[1])
        self.down = {0: [], 1: self.merge(inner, far)}
        self.from_up = {0: self.down[1], 1: far}
        self.from_down = {0: [], 1: first}
        own = lambda q: [(q, True, c) for c in range(CHUNKS)]
        narrow = lambda entries: [e for e in entries if e[1] and e[2] >= WIDE]
        self.cross = {
            0: own(0) + narrow(self.from_up[0]),
            1: own(1) + self.weave(narrow(self.from_down[1]), narrow(self.from_up[1])),
        }
        self.from_cross = {q: [(k, not same, c) for k, same, c in self.cross[q]] for q in (0, 1)}

    @staticmethod
    def merge(own, passed):
        return own + passed

    @staticmethod
    def weave(a, b):
        out = []
        for i in range(max(len(a), len(b))):
            out += a[i : i + 1] + b[i : i + 1]
        return out


class Weights:
    def __init__(self, lists, q):
        self.q = q
        self.out = {"up": list(lists.up[q]), "down": list(lists.down[q]), "cross": list(lists.cross[q])}
        self.into = {
            "cross": list(lists.from_cross[q]), "down": list(lists.from_down[q]), "up": list(lists.from_up[q]),
        }
        self.have = {(q, True, c) for c in range(CHUNKS)}
        self.got = {way: 0 for way in self.into}
        self.put = {way: 0 for way in self.out}

    def push(self, along, across):
        moves = []
        for way, goal in (("up", along), ("down", along), ("cross", across)):
            while self.put[way] < min(len(self.out[way]), goal):
                entry = self.out[way][self.put[way]]
                if entry not in self.have:
                    break
                moves.append(("send", way, entry))
                self.put[way] += 1
        return moves

    def take(self, along, across, push_along, push_across):
        moves = self.push(push_along, push_across)
        goals = {"cross": across, "down": along, "up": along}
        for count in range(1, max(along, across) + 1):
            for way, goal in goals.items():
                if self.got[way] < min(len(self.into[way]), goal, count):
                    entry = self.into[way][self.got[way]]
                    moves.append(("wait", way, entry))
                    self.have.add(entry)
                    self.got[way] += 1
                    moves += self.push(push_along, push_across)
        return moves

    def done(self):
        return all(self.got[w] == len(self.into[w]) for w in self.into) and all(
            self.put[w] == len(self.out[w]) for w in self.out
        )


def kernel(
    n, tp, heads,
    x_hbm, q_hbm, k_hbm, v_hbm, c_hbm, mix_hbm, gain_hbm, f_hbm, mom_hbm, w_hbm,
    wall, low, nm_ref, tot_ref,
    x_ref, q_ref, k_ref, v_ref, c_ref, mix_ref, gain_ref, f_ref, mom_ref, w_ref,
    fall, nmall, fwide, dq, dv, psend, precv, pside, pmid, sums,
    l_sem, f_send, f_recv, s_send, s_recv, w_send, w_recv, n_send, n_recv, p_send, p_recv, t_send, t_recv,
):
    me = lax.axis_index("fs")
    mt = lax.axis_index("tp")
    depth = fall.shape[0]
    deep = depth // n
    rank = fall.shape[1] // 2
    rank_here = rank // n
    cols = dq.shape[1]
    tiles_f, tiles_w = rank // LANES, cols // LANES
    per_row = 2 * tiles_w

    local = {}
    for i, (name, src, dst) in enumerate((
        ("f", f_hbm, f_ref), ("w", w_hbm, w_ref), ("gain", gain_hbm, gain_ref), ("mix", mix_hbm, mix_ref),
        ("q", q_hbm, q_ref), ("k", k_hbm, k_ref), ("v", v_hbm, v_ref), ("c", c_hbm, c_ref),
        ("x", x_hbm, x_ref), ("mom", mom_hbm, mom_ref),
    )):
        local[name] = pltpu.make_async_copy(src, dst, l_sem.at[i])
        local[name].start()

    barrier = pltpu.get_barrier_semaphore()
    for hop in range(1, n):
        pl.semaphore_signal(barrier, inc=1, device_id={"fs": (me + hop) % n}, device_id_type=MESH)
    for hop in range(1, tp):
        pl.semaphore_signal(barrier, inc=1, device_id={"tp": (mt + hop) % tp}, device_id_type=MESH)

    local["f"].wait()
    fwide[...] = f_ref[...].astype(jnp.float32)
    here = pl.ds(pl.multiple_of(me * deep, deep), deep)
    for t in range(2 * tiles_f):
        fall[here, t * LANES : (t + 1) * LANES] = split(fwide, t, tiles_f, deep).astype(jnp.bfloat16)
    local["w"].wait()
    wall[pl.ds(pl.multiple_of(me * deep * per_row, 16), deep * per_row), :] = w_ref[...].astype(jnp.bfloat16)
    for name in ("gain", "mix", "q", "k", "v", "c"):
        local[name].wait()

    def head(i):
        head_step(i, q_ref, k_ref, v_ref, c_ref, mix_ref, gain_ref, dq, dv)

    def remote(src, send, recv, axis, target):
        return pltpu.make_async_remote_copy(
            src_ref=src, dst_ref=src, send_sem=send, recv_sem=recv, device_id={axis: target}, device_id_type=MESH
        )

    def project():
        local["x"].wait()
        for m, cot in enumerate((dq, dv)):
            reduced = jnp.dot(
                x_ref[...], fall[:, m * rank : (m + 1) * rank], preferred_element_type=jnp.float32
            ).astype(jnp.bfloat16)
            partial = lax.dot_general(
                reduced, cot[...], (((0,), (0,)), ((), ())), preferred_element_type=jnp.float32
            )
            for j in range(n):
                psend[j, m] = partial[j * rank_here : (j + 1) * rank_here].astype(psend.dtype)

    def p_copy(hop):
        peer = (me + hop) % n
        return pltpu.make_async_remote_copy(
            src_ref=psend.at[peer], dst_ref=precv.at[hop], send_sem=p_send.at[hop], recv_sem=p_recv.at[hop],
            device_id={"fs": peer}, device_id_type=MESH,
        )

    def momentum(total):
        local["mom"].wait()
        length = x_ref.shape[0]
        for t in range(2 * tiles_w):
            m, lanes = t // tiles_w, slice(t % tiles_w * LANES, (t % tiles_w + 1) * LANES)
            moments = BETA * split(mom_ref, t, tiles_w, rank_here)
            moments += total[m, :, lanes] * (length * n) ** (-0.5)
            nm_ref[pl.ds(t % tiles_w * 2 + m, rank_here, stride=per_row), :] = moments
            nmall[me, m, :, lanes] = moments.astype(nmall.dtype)

    def t_copy(hop):
        return pltpu.make_async_remote_copy(
            src_ref=sums.at[0], dst_ref=sums.at[hop], send_sem=t_send.at[hop], recv_sem=t_recv.at[hop],
            device_id={"tp": (mt + hop) % tp}, device_id_type=MESH,
        )

    def squares():
        everything = nmall[...].astype(jnp.float32)
        parts = jnp.sum(jnp.sum(everything * everything, axis=0), axis=1)
        sums[0] = jnp.sum(parts, axis=1, keepdims=True) + jnp.zeros((2, LANES), jnp.float32)
        for hop in range(1, tp):
            t_copy(hop).start()

    def totals():
        result = sums[0]
        for hop in range(1, tp):
            t_copy(hop).wait_recv()
            result += sums[hop]
        tot_ref[...] = result

    def lows(start, count):
        for m in range(2):
            block = nmall[:, m].reshape(rank, cols).astype(jnp.bfloat16)
            product = jnp.dot(
                fall[start : start + count, m * rank : (m + 1) * rank], block, preferred_element_type=jnp.float32
            )
            for t in range(tiles_w):
                low[pl.ds(start * per_row + 2 * t + m, count, stride=per_row), :] = (
                    product[:, t * LANES : (t + 1) * LANES]
                )

    def weights(index, chunk, chunks):
        size = deep // chunks * per_row
        return wall.at[pl.ds(pl.multiple_of(index * deep * per_row + chunk * size, 16), size)]

    quarter = 2 * rank // tp
    if n == 8 and tp == 4 and quarter % LANES == 0 and deep % (2 * CHUNKS) == 0:
        place, parity = me // 2, me % 2
        flip = place // 2
        side = jnp.where(flip == 0, place, 3 - place)
        lists = Lists()
        states = [Weights(lists, q) for q in (0, 1)]
        partner = me + 1 - 2 * parity
        far, near = (mt + 2) % tp, mt + 1 - 2 * (mt % 2)

        def index_of(k, same):
            return 2 * (k + flip * (3 - 2 * k)) + (parity if same else 1 - parity)

        def target(q, way):
            return partner if way == "cross" else index_of(q + 1 if way == "up" else q - 1, True)

        ways = {"up": 0, "down": 1, "cross": 2}

        def w_copy(q, way, entry):
            k, same, chunk = entry
            index = index_of(k, same)
            return remote(
                weights(index, chunk, CHUNKS), w_send.at[index, chunk, ways[way]], w_recv.at[index, chunk],
                "fs", target(q, way),
            )

        def run(q, moves):
            for kind, way, entry in moves:
                if kind == "send":
                    w_copy(q, way, entry).start()
                else:
                    w_copy(q, "cross", entry).wait_recv()

        def piece(index, which):
            return fall.at[
                pl.ds(pl.multiple_of(index * deep, deep), deep), pl.ds(pl.multiple_of(which * quarter, quarter), quarter)
            ]

        def others(q):
            return sorted((k for k in range(4) if k != q), key=lambda k: (abs(k - q), k))

        def small(kind, index, way, to):
            if kind == "f":
                return remote(piece(index, mt), f_send.at[index, way], f_recv.at[index], "fs", to)
            return remote(nmall.at[index], n_send.at[index, way], n_recv.at[index], "fs", to)

        def small_begin(kind, q):
            for i, k in enumerate(reversed(others(q))):
                small(kind, me, i, index_of(k, True)).start()
                if kind in DIRECT:
                    small(kind, me, 4 + i, index_of(k, False)).start()
            small(kind, me, 3, partner).start()

        def spread(index, which, to, way):
            return remote(piece(index, which), s_send.at[index, way], s_recv.at[index, way], "tp", to)

        def small_wait(kind, q, k, same):
            index = index_of(k, same)
            small(kind, index, 0, partner).wait_recv()
            if same and kind not in DIRECT:
                small(kind, index, 0, partner).start()
            if kind == "f":
                spread(index, mt, far, 0).start()
                spread(index, mt, near, 1).start()

        def pieces(q):
            return [(q, False)] + [(k, True) for k in others(q)] + [(k, False) for k in others(q)]

        def place_of(k):
            return k + flip * (3 - 2 * k)

        def p_order(q):
            return list(reversed(others(q))) + [q]

        def p_across(index, at):
            return pltpu.make_async_remote_copy(
                src_ref=psend.at[index], dst_ref=pside.at[at], send_sem=p_send.at[at], recv_sem=p_recv.at[at],
                device_id={"fs": partner}, device_id_type=MESH,
            )

        def p_along(q, k):
            return pltpu.make_async_remote_copy(
                src_ref=pmid.at[place_of(k)], dst_ref=precv.at[place], send_sem=p_send.at[4 + place_of(k)],
                recv_sem=p_recv.at[4 + place], device_id={"fs": index_of(k, True)}, device_id_type=MESH,
            )

        def gathered():
            total = psend[me].astype(jnp.float32) + pside[place].astype(jnp.float32)
            for hop in range(1, 4):
                at = (place + hop) % 4
                pltpu.make_async_remote_copy(
                    src_ref=pmid.at[at], dst_ref=precv.at[at], send_sem=p_send.at[4 + at], recv_sem=p_recv.at[4 + at],
                    device_id={"fs": partner}, device_id_type=MESH,
                ).wait_recv()
                total += precv[at].astype(jnp.float32)
            return total

        def segment(tokens):
            for q in (0, 1):

                @pl.when(side == q)
                def _(q=q):
                    for token in tokens:
                        kind, *rest = token
                        if kind == "w":
                            run(q, states[q].take(*rest))
                        elif kind == "begin":
                            small_begin(rest[0], q)
                        elif kind == "px":
                            for k in p_order(q):
                                p_across(index_of(k, False), place_of(k)).start()
                        elif kind == "pz":
                            for i in rest[0]:
                                k = p_order(q)[i]
                                p_across(index_of(k, True), place_of(k)).wait_recv()
                                if k != q:
                                    pmid[place_of(k)] = (
                                        psend[index_of(k, True)].astype(jnp.float32)
                                        + pside[place_of(k)].astype(jnp.float32)
                                    ).astype(pmid.dtype)
                                    p_along(q, k).start()
                        elif kind == "small":
                            for i in rest[1]:
                                small_wait(rest[0], q, *pieces(q)[i])
                        elif kind == "all":
                            along, across, ahead = rest
                            while not states[q].done():
                                run(q, states[q].take(along, across, along + ahead, across + ahead))
                                along, across = along + 1, across + 1
                        elif kind == "spread":
                            for k, same in pieces(q):
                                index = index_of(k, same)
                                spread(index, far, far, 0).wait_recv()
                                spread(index, far, near, 2).start()
                            for k, same in pieces(q):
                                index = index_of(k, same)
                                spread(index, near, near, 1).wait_recv()
                                spread(index, (near + 2) % tp, near, 2).wait_recv()
                        elif kind == "sent":
                            for way in ways:
                                for entry in states[q].out[way]:
                                    w_copy(q, way, entry).wait_send()
                            for name in ("f", "n"):
                                for way in range(7 if name in DIRECT else 4):
                                    small(name, me, way, partner).wait_send()
                                for k in () if name in DIRECT else others(q):
                                    small(name, index_of(k, True), 0, partner).wait_send()
                            for k in range(4):
                                p_across(index_of(k, False), place_of(k)).wait_send()
                                if k != q:
                                    p_along(q, k).wait_send()
                            for k, same in pieces(q):
                                for way in range(3):
                                    spread(index_of(k, same), mt, near, way).wait_send()

        computes = {
            "project": project, "squares": squares, "totals": totals, "momentum": lambda: momentum(gathered()),
            "lows": lambda j: lows(j * deep, deep),
        }
        head(0)
        pl.semaphore_wait(barrier, n - 1 + tp - 1)
        for token in SCHEDULE:
            if token[0] == "head":
                for i in range(token[1], heads if token[1] == 3 else token[1] + 1):
                    head(i)
            elif token[0] in computes:
                computes[token[0]](*token[1:])
            else:
                segment([token])
        segment([("sent",)])
    else:
        for i in range(heads):
            head(i)
        pl.semaphore_wait(barrier, n - 1 + tp - 1)

        def block(kind, index, hop):
            if kind == "f":
                return remote(
                    fall.at[pl.ds(pl.multiple_of(index * deep, 8), deep)], f_send.at[hop], f_recv.at[index],
                    "fs", (me + hop) % n,
                )
            if kind == "w":
                return remote(weights(index, 0, 1), w_send.at[hop], w_recv.at[index], "fs", (me + hop) % n)
            return remote(nmall.at[index], n_send.at[hop], n_recv.at[index], "fs", (me + hop) % n)

        def each(action):
            def step(hop, carry):
                action(hop)
                return carry

            lax.fori_loop(1, n, step, 0)

        each(lambda hop: block("f", me, hop).start())
        each(lambda hop: block("w", me, hop).start())
        each(lambda hop: block("f", (me + hop) % n, hop).wait_recv())
        project()
        each(lambda hop: p_copy(hop).start())

        def add(hop, total):
            p_copy(hop).wait_recv()
            return total + precv[hop].astype(jnp.float32)

        momentum(lax.fori_loop(1, n, add, psend[me].astype(jnp.float32)))
        each(lambda hop: block("n", me, hop).start())
        each(lambda hop: block("n", (me + hop) % n, hop).wait_recv())
        squares()
        for start in range(0, depth, 256):
            lows(start, min(256, depth - start))
        totals()
        each(lambda hop: block("w", (me + hop) % n, hop).wait_recv())
        for kind in ("f", "w", "n"):
            each(lambda hop, kind=kind: block(kind, me, hop).wait_send())
        each(lambda hop: p_copy(hop).wait_send())
    for hop in range(1, tp):
        t_copy(hop).wait_send()


def finish(n, entries, wall, low, nm_ref, tot_ref, step_hbm, nm_hbm, copies_hbm, step, copies, sems):
    me = lax.axis_index("fs")
    rows = low.shape[0]
    own = rows // n
    nm_copy = pltpu.make_async_copy(nm_ref, nm_hbm, sems.at[0])
    nm_copy.start()
    rate = RATE_BASE / jnp.sqrt(1.0 + tot_ref[...] / entries)
    count = min(rows // 16, 1024)
    odd = lax.broadcasted_iota(jnp.int32, (count, LANES), 0) % 2 == 1
    rates = jnp.where(odd, rate[1:2], rate[0:1])
    started = [nm_copy]
    for i in range(0, own, min(count, own)):
        size = min(count, own)
        start = pl.multiple_of(me * own + i, 8)
        step[i : i + size, :] = low[pl.ds(start, size), :] * rates[:size]
    started.append(pltpu.make_async_copy(step, step_hbm, sems.at[1]))
    started[-1].start()
    for i in range(rows // count):
        at = slice(i * count, (i + 1) * count)
        copies[at, :] = (wall[at, :].astype(jnp.float32) - low[at, :] * rates).astype(jnp.bfloat16)
        started.append(pltpu.make_async_copy(copies.at[at], copies_hbm.at[at], sems.at[2 + i]))
        started[-1].start()
    for copy in started:
        copy.wait()


def to_rows(array):
    rows, maps, cols = array.shape
    return array.reshape(rows, maps, cols // LANES, LANES).transpose(0, 2, 1, 3).reshape(-1, LANES)


def from_rows(array, rows):
    return (
        array.reshape(rows, -1, 2, LANES).transpose(0, 2, 1, 3).reshape(rows, 2, -1)
    )


def per_device(
    n, tp, inputs, queries, keys, values, head_cot, mixing, head_gain, factors, moments, weights
):
    length, depth = inputs.shape
    heads = mixing.shape[0]
    deep, _, rank = factors.shape
    rank_here, _, cols = moments.shape
    wire = jnp.bfloat16 if rank_here % 16 == 0 else jnp.float32
    per_row = 2 * cols // LANES
    hbm = pl.BlockSpec(memory_space=pltpu.HBM)
    vmem = pl.BlockSpec(memory_space=pltpu.VMEM)
    dma = pltpu.SemaphoreType.DMA
    args = (
        inputs, queries, keys, values, head_cot, mixing, head_gain[None, :],
        to_rows(factors), to_rows(moments), to_rows(weights),
    )
    held = pl.pallas_call(
        functools.partial(kernel, n, tp, heads),
        out_shape=(
            pltpu.VMEM((depth * per_row, LANES), jnp.bfloat16),
            pltpu.VMEM((depth * per_row, LANES), jnp.float32),
            pltpu.VMEM((rank_here * per_row, LANES), jnp.float32),
            pltpu.VMEM((2, LANES), jnp.float32),
        ),
        in_specs=[hbm] * len(args),
        out_specs=(vmem,) * 4,
        scratch_shapes=[
            pltpu.VMEM((length, depth), jnp.bfloat16),
            pltpu.VMEM((length, cols), jnp.bfloat16),
            pltpu.VMEM((length, cols), jnp.bfloat16),
            pltpu.VMEM((length, cols), jnp.bfloat16),
            pltpu.VMEM((length, cols), jnp.bfloat16),
            pltpu.SMEM((heads,), jnp.float32),
            pltpu.VMEM((1, head_gain.shape[0]), jnp.float32),
            pltpu.VMEM((deep * 2 * rank // LANES, LANES), jnp.bfloat16),
            pltpu.VMEM((rank_here * per_row, LANES), jnp.float32),
            pltpu.VMEM((deep * per_row, LANES), jnp.float32),
            pltpu.VMEM((depth, 2 * rank), jnp.bfloat16),
            pltpu.VMEM((n, 2, rank_here, cols), wire),
            pltpu.VMEM((deep * 2 * rank // LANES, LANES), jnp.float32),
            pltpu.VMEM((length, cols), jnp.bfloat16),
            pltpu.VMEM((length, cols), jnp.bfloat16),
            pltpu.VMEM((n, 2, rank_here, cols), wire),
            pltpu.VMEM((n, 2, rank_here, cols), wire),
            pltpu.VMEM((4, 2, rank_here, cols), wire),
            pltpu.VMEM((4, 2, rank_here, cols), wire),
            pltpu.VMEM((tp, 2, LANES), jnp.float32),
            dma((len(args),)),
            *(
                (
                    dma((n, 7)), dma((n,)), dma((n, 3)), dma((n, 3)),
                    dma((n, CHUNKS, 3)), dma((n, CHUNKS)), dma((n, 7)), dma((n,)),
                )
                if n == 8
                else (dma((n,)), dma((n,)), dma((1,)), dma((1,)), dma((n,)), dma((n,)), dma((n,)), dma((n,)))
            ),
            dma((n,)), dma((n,)),
            dma((tp,)), dma((tp,)),
        ],
        compiler_params=pltpu.CompilerParams(
            collective_id=0, has_side_effects=True, vmem_limit_bytes=36 * 1024 * 1024
        ),
    )(*(pltpu.with_memory_space_constraint(arg, pltpu.HBM) for arg in args))
    out_hbm = pl.BlockSpec(memory_space=pltpu.HBM)
    step, new_moments, copies = pl.pallas_call(
        functools.partial(finish, n, rank * cols * tp),
        out_shape=(
            jax.ShapeDtypeStruct((deep * per_row, LANES), jnp.float32),
            jax.ShapeDtypeStruct((rank_here * per_row, LANES), jnp.float32),
            jax.ShapeDtypeStruct((depth * per_row, LANES), jnp.bfloat16),
        ),
        in_specs=[vmem] * 4,
        out_specs=(out_hbm,) * 3,
        scratch_shapes=[
            pltpu.VMEM((deep * per_row, LANES), jnp.float32),
            pltpu.VMEM((depth * per_row, LANES), jnp.bfloat16),
            dma((18,)),
        ],
        compiler_params=pltpu.CompilerParams(vmem_limit_bytes=16 * 1024 * 1024),
    )(*held)
    return from_rows(step, deep), from_rows(new_moments, rank_here), from_rows(copies, depth)


def solution(mesh):
    placed = (
        P("fs", None),
        P("fs", "tp"),
        P("fs", "tp"),
        P("fs", "tp"),
        P("fs", "tp"),
        P("tp"),
        P(),
        P("fs", None, None),
        P("fs", None, "tp"),
        P("fs", None, "tp"),
    )
    return jax.shard_map(
        functools.partial(per_device, mesh.shape["fs"], mesh.shape["tp"]),
        mesh=mesh,
        in_specs=placed,
        out_specs=(P("fs", None, "tp"), P("fs", None, "tp"), P(None, None, "tp")),
        check_vma=False,
    )
```

```python
import functools

import jax
import jax.numpy as jnp
from jax import lax
from jax.experimental import pallas as pl
from jax.experimental.pallas import tpu as pltpu
from jax.sharding import PartitionSpec as P

EPS = 0.05
BETA = 0.9
RATE_BASE = 0.5
MESH = pl.DeviceIdType.MESH
LANES = 128
CHUNKS = 8
WIDE = 2
SCHEDULE = [
    ("begin", "f"), ("own",), ("w", 0, 0, 4, 2), ("head", 0), ("head", 1),
    ("small", "f", (0,)), ("w", 0, 0, 5, 2),
    ("head", 2),
    ("small", "f", (1, 2)), ("w", 0, 0, 10, 2),
    ("head", 3),
    ("small", "f", (3,)), ("w", 0, 0, 10, 8), ("small", "f", (4, 5, 6)), ("spread",),
    ("w", 6, 6, 12, 10),
    ("project",),
    ("px",), ("w", 8, 8, 14, 10), ("w", 9, 8, 15, 10),
    ("pz", (0,)), ("w", 10, 8, 15, 10), ("pz", (1,)), ("w", 11, 8, 15, 11), ("pz", (2,)), ("pz", (3,)),
    ("w", 12, 9, 15, 12), ("w", 13, 10, 16, 13), ("w", 14, 11, 17, 14),
    ("momentum",),
    ("begin", "n"), ("w", 14, 11, 17, 14), ("w", 15, 12, 18, 15), ("w", 16, 13, 19, 16),
    ("small", "n", (0,)), ("small", "n", (1,)), ("w", 17, 14, 20, 16), ("small", "n", (2,)), ("w", 18, 14, 21, 16),
    ("small", "n", (3,)), ("w", 19, 15, 22, 17), ("small", "n", (4,)), ("w", 20, 15, 23, 18), ("small", "n", (5,)),
    ("w", 21, 16, 24, 19),
    ("small", "n", (6,)),
    ("squares",),
]
for j in range(8):
    SCHEDULE += [("lows", j), ("w", 22 + j, 17 + j, 25 + j, 20 + j)]
SCHEDULE += [("totals",), ("all", 30, 25, 3)]


def split(ref, t, tiles, count):
    return ref[pl.ds(t % tiles * 2 + t // tiles, count, stride=2 * tiles), :]


def head_step(head, q_ref, k_ref, v_ref, c_ref, mix_ref, gain_ref, dq_ref, dv_ref):
    length = q_ref.shape[0]
    width = gain_ref.shape[1]
    half = width // 2
    factor = half ** (-0.5)
    cols = slice(head * width, (head + 1) * width)
    query, key, value = q_ref[:, cols], k_ref[:, cols], v_ref[:, cols]
    lane = lax.broadcasted_iota(jnp.int32, (length, width), 1)
    zero = jnp.zeros_like(key)
    key0 = jnp.where(lane < half, key, zero)
    key1 = jnp.where(lane < half, zero, key)
    row = lax.broadcasted_iota(jnp.int32, (length, length), 0)
    col = lax.broadcasted_iota(jnp.int32, (length, length), 1)
    causal = col <= row
    mix = mix_ref[head]
    nt = (((1,), (1,)), ((), ()))
    tn = (((0,), (0,)), ((), ()))

    def probs(rows):
        scores = lax.dot_general(query, rows, nt, preferred_element_type=jnp.float32) * factor
        scores = jnp.where(causal, scores, -jnp.inf)
        expo = jnp.exp(scores - jnp.max(scores, axis=-1, keepdims=True))
        return expo * (1.0 / jnp.sum(expo, axis=-1, keepdims=True))

    first, second = probs(key0), probs(key1)
    mixed = (first - mix * second).astype(jnp.bfloat16)
    output = jnp.dot(mixed, value, preferred_element_type=jnp.float32)
    inverse = lax.rsqrt(jnp.mean(output * output, axis=-1, keepdims=True) + EPS)
    scaled = gain_ref[...] * c_ref[:, cols].astype(jnp.float32)
    d_out = inverse * scaled - output * (inverse * inverse * inverse) * jnp.mean(
        output * scaled, axis=-1, keepdims=True
    )
    d_out = d_out.astype(jnp.bfloat16)
    dv_ref[:, cols] = lax.dot_general(mixed, d_out, tn, preferred_element_type=jnp.float32).astype(jnp.bfloat16)
    d_mix = lax.dot_general(d_out, value, nt, preferred_element_type=jnp.float32)
    d_first = first * (d_mix - jnp.sum(first * d_mix, axis=-1, keepdims=True))
    d_second = -mix * second * (d_mix - jnp.sum(second * d_mix, axis=-1, keepdims=True))
    d_query = jnp.dot(d_first.astype(jnp.bfloat16), key0, preferred_element_type=jnp.float32)
    d_query += jnp.dot(d_second.astype(jnp.bfloat16), key1, preferred_element_type=jnp.float32)
    dq_ref[:, cols] = (d_query * factor).astype(jnp.bfloat16)


class Lists:
    def __init__(self):
        def source(k, order):
            return [(k, True, c) for c in order] + [(k, False, c) for c in range(WIDE)]

        order = list(range(WIDE, CHUNKS)) + list(range(WIDE))
        mirror = lambda entries: [(3 - k, same, c) for k, same, c in entries]
        first = source(0, order)
        inner = source(1, order)
        self.up = {0: first, 1: self.merge(inner, first)}
        far = mirror(self.up[1])
        self.down = {0: [], 1: self.merge(inner, far)}
        self.from_up = {0: self.down[1], 1: far}
        self.from_down = {0: [], 1: first}
        own = lambda q: [(q, True, c) for c in range(CHUNKS)]
        narrow = lambda entries: [e for e in entries if e[1] and e[2] >= WIDE]
        self.cross = {
            0: own(0) + narrow(self.from_up[0]),
            1: own(1) + self.weave(narrow(self.from_down[1]), narrow(self.from_up[1])),
        }
        self.from_cross = {q: [(k, not same, c) for k, same, c in self.cross[q]] for q in (0, 1)}

    @staticmethod
    def merge(own, passed):
        return own + passed

    @staticmethod
    def weave(a, b):
        out = []
        for i in range(max(len(a), len(b))):
            out += a[i : i + 1] + b[i : i + 1]
        return out


class Weights:
    def __init__(self, lists, q):
        self.q = q
        self.out = {"up": list(lists.up[q]), "down": list(lists.down[q]), "cross": list(lists.cross[q])}
        self.into = {
            "cross": list(lists.from_cross[q]), "down": list(lists.from_down[q]), "up": list(lists.from_up[q]),
        }
        self.have = {(q, True, c) for c in range(CHUNKS)}
        self.got = {way: 0 for way in self.into}
        self.put = {way: 0 for way in self.out}

    def push(self, along, across):
        moves = []
        for way, goal in (("up", along), ("down", along), ("cross", across)):
            while self.put[way] < min(len(self.out[way]), goal):
                entry = self.out[way][self.put[way]]
                if entry not in self.have:
                    break
                moves.append(("send", way, entry))
                self.put[way] += 1
        return moves

    def take(self, along, across, push_along, push_across):
        moves = self.push(push_along, push_across)
        goals = {"cross": across, "down": along, "up": along}
        for count in range(1, max(along, across) + 1):
            for way, goal in goals.items():
                if self.got[way] < min(len(self.into[way]), goal, count):
                    entry = self.into[way][self.got[way]]
                    moves.append(("wait", way, entry))
                    self.have.add(entry)
                    self.got[way] += 1
                    moves += self.push(push_along, push_across)
        return moves

    def done(self):
        return all(self.got[w] == len(self.into[w]) for w in self.into) and all(
            self.put[w] == len(self.out[w]) for w in self.out
        )


def kernel(
    n, tp, heads,
    x_hbm, q_hbm, k_hbm, v_hbm, c_hbm, mix_hbm, gain_hbm, f_hbm, mom_hbm, w_hbm,
    wall, low, nm_ref, tot_ref,
    x_ref, q_ref, k_ref, v_ref, c_ref, mix_ref, gain_ref, f_ref, mom_ref, w_ref,
    fall, nmall, fwide, dq, dv, psend, precv, pside, pmid, sums,
    l_sem, f_send, f_recv, s_send, s_recv, w_send, w_recv, n_send, n_recv, p_send, p_recv, t_send, t_recv,
):
    me = lax.axis_index("fs")
    mt = lax.axis_index("tp")
    depth = fall.shape[0]
    deep = depth // n
    rank = fall.shape[1] // 2
    rank_here = rank // n
    cols = dq.shape[1]
    tiles_f, tiles_w = rank // LANES, cols // LANES
    per_row = 2 * tiles_w

    local = {}
    for i, (name, src, dst) in enumerate((
        ("f", f_hbm, f_ref), ("w", w_hbm, w_ref), ("gain", gain_hbm, gain_ref), ("mix", mix_hbm, mix_ref),
        ("q", q_hbm, q_ref), ("k", k_hbm, k_ref), ("v", v_hbm, v_ref), ("c", c_hbm, c_ref),
        ("x", x_hbm, x_ref), ("mom", mom_hbm, mom_ref),
    )):
        local[name] = pltpu.make_async_copy(src, dst, l_sem.at[i])
        local[name].start()

    barrier = pltpu.get_barrier_semaphore()
    for hop in range(1, n):
        pl.semaphore_signal(barrier, inc=1, device_id={"fs": (me + hop) % n}, device_id_type=MESH)
    for hop in range(1, tp):
        pl.semaphore_signal(barrier, inc=1, device_id={"tp": (mt + hop) % tp}, device_id_type=MESH)

    local["f"].wait()
    fwide[...] = f_ref[...].astype(jnp.float32)
    here = pl.ds(pl.multiple_of(me * deep, deep), deep)
    for t in range(2 * tiles_f):
        fall[here, t * LANES : (t + 1) * LANES] = split(fwide, t, tiles_f, deep).astype(jnp.bfloat16)

    def own_weights():
        local["w"].wait()
        wall[pl.ds(pl.multiple_of(me * deep * per_row, 16), deep * per_row), :] = w_ref[...].astype(jnp.bfloat16)

    def head(i):
        if i == 0:
            for name in ("gain", "mix", "q", "k", "v", "c"):
                local[name].wait()
        head_step(i, q_ref, k_ref, v_ref, c_ref, mix_ref, gain_ref, dq, dv)

    def remote(src, send, recv, axis, target):
        return pltpu.make_async_remote_copy(
            src_ref=src, dst_ref=src, send_sem=send, recv_sem=recv, device_id={axis: target}, device_id_type=MESH
        )

    def project():
        local["x"].wait()
        for m, cot in enumerate((dq, dv)):
            reduced = jnp.dot(
                x_ref[...], fall[:, m * rank : (m + 1) * rank], preferred_element_type=jnp.float32
            ).astype(jnp.bfloat16)
            partial = lax.dot_general(
                reduced, cot[...], (((0,), (0,)), ((), ())), preferred_element_type=jnp.float32
            )
            for j in range(n):
                psend[j, m] = partial[j * rank_here : (j + 1) * rank_here].astype(psend.dtype)

    def p_copy(hop):
        peer = (me + hop) % n
        return pltpu.make_async_remote_copy(
            src_ref=psend.at[peer], dst_ref=precv.at[hop], send_sem=p_send.at[hop], recv_sem=p_recv.at[hop],
            device_id={"fs": peer}, device_id_type=MESH,
        )

    def momentum(total):
        local["mom"].wait()
        length = x_ref.shape[0]
        for t in range(2 * tiles_w):
            m, lanes = t // tiles_w, slice(t % tiles_w * LANES, (t % tiles_w + 1) * LANES)
            moments = BETA * split(mom_ref, t, tiles_w, rank_here)
            moments += total[m, :, lanes] * (length * n) ** (-0.5)
            nm_ref[pl.ds(t % tiles_w * 2 + m, rank_here, stride=per_row), :] = moments
            nmall[me, m, :, lanes] = moments.astype(nmall.dtype)

    def t_copy(hop):
        return pltpu.make_async_remote_copy(
            src_ref=sums.at[0], dst_ref=sums.at[hop], send_sem=t_send.at[hop], recv_sem=t_recv.at[hop],
            device_id={"tp": (mt + hop) % tp}, device_id_type=MESH,
        )

    def squares():
        everything = nmall[...].astype(jnp.float32)
        parts = jnp.sum(jnp.sum(everything * everything, axis=0), axis=1)
        sums[0] = jnp.sum(parts, axis=1, keepdims=True) + jnp.zeros((2, LANES), jnp.float32)
        for hop in range(1, tp):
            t_copy(hop).start()

    def totals():
        result = sums[0]
        for hop in range(1, tp):
            t_copy(hop).wait_recv()
            result += sums[hop]
        tot_ref[...] = result

    def lows(start, count):
        for m in range(2):
            block = nmall[:, m].reshape(rank, cols).astype(jnp.bfloat16)
            product = jnp.dot(
                fall[start : start + count, m * rank : (m + 1) * rank], block, preferred_element_type=jnp.float32
            )
            for t in range(tiles_w):
                low[pl.ds(start * per_row + 2 * t + m, count, stride=per_row), :] = (
                    product[:, t * LANES : (t + 1) * LANES]
                )

    def weights(index, chunk, chunks):
        size = deep // chunks * per_row
        return wall.at[pl.ds(pl.multiple_of(index * deep * per_row + chunk * size, 16), size)]

    quarter = 2 * rank // tp
    if n == 8 and tp == 4 and quarter % LANES == 0 and deep % (2 * CHUNKS) == 0:
        place, parity = me // 2, me % 2
        flip = place // 2
        side = jnp.where(flip == 0, place, 3 - place)
        lists = Lists()
        states = [Weights(lists, q) for q in (0, 1)]
        partner = me + 1 - 2 * parity
        far, near = (mt + 2) % tp, mt + 1 - 2 * (mt % 2)

        def index_of(k, same):
            return 2 * (k + flip * (3 - 2 * k)) + (parity if same else 1 - parity)

        def target(q, way):
            return partner if way == "cross" else index_of(q + 1 if way == "up" else q - 1, True)

        ways = {"up": 0, "down": 1, "cross": 2}

        def w_copy(q, way, entry):
            k, same, chunk = entry
            index = index_of(k, same)
            return remote(
                weights(index, chunk, CHUNKS), w_send.at[ways[way]], w_recv.at[index, chunk],
                "fs", target(q, way),
            )

        def run(q, moves):
            for kind, way, entry in moves:
                if kind == "send":
                    w_copy(q, way, entry).start()
                else:
                    w_copy(q, "cross", entry).wait_recv()

        def piece(index, which):
            return fall.at[
                pl.ds(pl.multiple_of(index * deep, deep), deep), pl.ds(pl.multiple_of(which * quarter, quarter), quarter)
            ]

        def others(q):
            return sorted((k for k in range(4) if k != q), key=lambda k: (abs(k - q), k))

        def small(kind, index, to):
            if kind == "f":
                return remote(piece(index, mt), f_send.at[0], f_recv.at[index], "fs", to)
            return remote(nmall.at[index], n_send.at[0], n_recv.at[index], "fs", to)

        def small_begin(kind, q):
            for i, k in enumerate(reversed(others(q))):
                small(kind, me, index_of(k, True)).start()
            small(kind, me, partner).start()

        def spread(index, which, to, way):
            return remote(piece(index, which), s_send.at[0], s_recv.at[index, way], "tp", to)

        def small_wait(kind, q, k, same):
            index = index_of(k, same)
            small(kind, index, partner).wait_recv()
            if same:
                small(kind, index, partner).start()
            if kind == "f":
                spread(index, mt, far, 0).start()
                spread(index, mt, near, 1).start()

        def pieces(q):
            return [(q, False)] + [(k, True) for k in others(q)] + [(k, False) for k in others(q)]

        def place_of(k):
            return k + flip * (3 - 2 * k)

        def p_order(q):
            return list(reversed(others(q))) + [q]

        def p_across(index, at):
            return pltpu.make_async_remote_copy(
                src_ref=psend.at[index], dst_ref=pside.at[at], send_sem=p_send.at[0], recv_sem=p_recv.at[at],
                device_id={"fs": partner}, device_id_type=MESH,
            )

        def p_along(q, k):
            return pltpu.make_async_remote_copy(
                src_ref=pmid.at[place_of(k)], dst_ref=precv.at[place], send_sem=p_send.at[1],
                recv_sem=p_recv.at[4 + place], device_id={"fs": index_of(k, True)}, device_id_type=MESH,
            )

        def gathered():
            total = psend[me].astype(jnp.float32) + pside[place].astype(jnp.float32)
            for hop in range(1, 4):
                at = (place + hop) % 4
                pltpu.make_async_remote_copy(
                    src_ref=pmid.at[at], dst_ref=precv.at[at], send_sem=p_send.at[1], recv_sem=p_recv.at[4 + at],
                    device_id={"fs": partner}, device_id_type=MESH,
                ).wait_recv()
                total += precv[at].astype(jnp.float32)
            return total

        def segment(tokens):
            for q in (0, 1):

                @pl.when(side == q)
                def _(q=q):
                    for token in tokens:
                        kind, *rest = token
                        if kind == "w":
                            run(q, states[q].take(*rest))
                        elif kind == "begin":
                            small_begin(rest[0], q)
                        elif kind == "px":
                            for k in p_order(q):
                                p_across(index_of(k, False), place_of(k)).start()
                        elif kind == "pz":
                            for i in rest[0]:
                                k = p_order(q)[i]
                                p_across(index_of(k, True), place_of(k)).wait_recv()
                                if k != q:
                                    pmid[place_of(k)] = (
                                        psend[index_of(k, True)].astype(jnp.float32)
                                        + pside[place_of(k)].astype(jnp.float32)
                                    ).astype(pmid.dtype)
                                    p_along(q, k).start()
                        elif kind == "small":
                            for i in rest[1]:
                                small_wait(rest[0], q, *pieces(q)[i])
                        elif kind == "all":
                            along, across, ahead = rest
                            while not states[q].done():
                                run(q, states[q].take(along, across, along + ahead, across + ahead))
                                along, across = along + 1, across + 1
                        elif kind == "spread":
                            for k, same in pieces(q):
                                index = index_of(k, same)
                                spread(index, far, far, 0).wait_recv()
                                spread(index, far, near, 2).start()
                            for k, same in pieces(q):
                                index = index_of(k, same)
                                spread(index, near, near, 1).wait_recv()
                                spread(index, (near + 2) % tp, near, 2).wait_recv()
                        elif kind == "sent":
                            for way in ways:
                                if states[q].out[way]:
                                    all_sent(wall, w_send.at[ways[way]], len(states[q].out[way]), CHUNKS)

        def all_sent(whole, sem, count, per_block):
            rows = whole.shape[0] // n // per_block * count
            part = whole.at[pl.ds(0, rows)]
            remote(part, sem, sem, "fs", partner).wait_send()

        def rest_sent():
            all_sent(fall, f_send.at[0], 7, tp)
            all_sent(fall, s_send.at[0], 21, tp)
            all_sent(nmall, n_send.at[0], 7, 1)
            all_sent(psend, p_send.at[0], 4, 1)
            remote(pmid.at[pl.ds(0, 3)], p_send.at[1], p_send.at[1], "fs", partner).wait_send()

        computes = {
            "own": own_weights, "project": project, "squares": squares, "totals": totals, "momentum": lambda: momentum(gathered()),
            "lows": lambda j: lows(j * deep, deep),
        }
        pl.semaphore_wait(barrier, n - 1 + tp - 1)
        for token in SCHEDULE:
            if token[0] == "head":
                for i in range(token[1], heads if token[1] == 3 else token[1] + 1):
                    head(i)
            elif token[0] in computes:
                computes[token[0]](*token[1:])
            else:
                segment([token])
        segment([("sent",)])
        rest_sent()
    else:
        own_weights()
        for i in range(heads):
            head(i)
        pl.semaphore_wait(barrier, n - 1 + tp - 1)

        def block(kind, index, hop):
            if kind == "f":
                return remote(
                    fall.at[pl.ds(pl.multiple_of(index * deep, 8), deep)], f_send.at[hop], f_recv.at[index],
                    "fs", (me + hop) % n,
                )
            if kind == "w":
                return remote(weights(index, 0, 1), w_send.at[hop], w_recv.at[index], "fs", (me + hop) % n)
            return remote(nmall.at[index], n_send.at[hop], n_recv.at[index], "fs", (me + hop) % n)

        def each(action):
            def step(hop, carry):
                action(hop)
                return carry

            lax.fori_loop(1, n, step, 0)

        each(lambda hop: block("f", me, hop).start())
        each(lambda hop: block("w", me, hop).start())
        each(lambda hop: block("f", (me + hop) % n, hop).wait_recv())
        project()
        each(lambda hop: p_copy(hop).start())

        def add(hop, total):
            p_copy(hop).wait_recv()
            return total + precv[hop].astype(jnp.float32)

        momentum(lax.fori_loop(1, n, add, psend[me].astype(jnp.float32)))
        each(lambda hop: block("n", me, hop).start())
        each(lambda hop: block("n", (me + hop) % n, hop).wait_recv())
        squares()
        for start in range(0, depth, 256):
            lows(start, min(256, depth - start))
        totals()
        each(lambda hop: block("w", (me + hop) % n, hop).wait_recv())
        for kind in ("f", "w", "n"):
            each(lambda hop, kind=kind: block(kind, me, hop).wait_send())
        each(lambda hop: p_copy(hop).wait_send())
    for hop in range(1, tp):
        t_copy(hop).wait_send()


def finish(n, entries, wall, low, nm_ref, tot_ref, step_hbm, nm_hbm, copies_hbm, step, copies, sems):
    me = lax.axis_index("fs")
    rows = low.shape[0]
    own = rows // n
    nm_copy = pltpu.make_async_copy(nm_ref, nm_hbm, sems.at[0])
    nm_copy.start()
    rate = RATE_BASE / jnp.sqrt(1.0 + tot_ref[...] / entries)
    count = min(rows // 16, 1024)
    odd = lax.broadcasted_iota(jnp.int32, (count, LANES), 0) % 2 == 1
    rates = jnp.where(odd, rate[1:2], rate[0:1])
    started = [nm_copy]
    for i in range(0, own, min(count, own)):
        size = min(count, own)
        start = pl.multiple_of(me * own + i, 8)
        step[i : i + size, :] = low[pl.ds(start, size), :] * rates[:size]
    started.append(pltpu.make_async_copy(step, step_hbm, sems.at[1]))
    started[-1].start()
    for i in range(rows // count):
        at = slice(i * count, (i + 1) * count)
        copies[at, :] = (wall[at, :].astype(jnp.float32) - low[at, :] * rates).astype(jnp.bfloat16)
        started.append(pltpu.make_async_copy(copies.at[at], copies_hbm.at[at], sems.at[2 + i]))
        started[-1].start()
    for copy in started:
        copy.wait()


def to_rows(array):
    rows, maps, cols = array.shape
    return array.reshape(rows, maps, cols // LANES, LANES).transpose(0, 2, 1, 3).reshape(-1, LANES)


def from_rows(array, rows):
    return (
        array.reshape(rows, -1, 2, LANES).transpose(0, 2, 1, 3).reshape(rows, 2, -1)
    )


def per_device(
    n, tp, inputs, queries, keys, values, head_cot, mixing, head_gain, factors, moments, weights
):
    length, depth = inputs.shape
    heads = mixing.shape[0]
    deep, _, rank = factors.shape
    rank_here, _, cols = moments.shape
    wire = jnp.bfloat16 if rank_here % 16 == 0 else jnp.float32
    per_row = 2 * cols // LANES
    hbm = pl.BlockSpec(memory_space=pltpu.HBM)
    vmem = pl.BlockSpec(memory_space=pltpu.VMEM)
    dma = pltpu.SemaphoreType.DMA
    args = (
        inputs, queries, keys, values, head_cot, mixing, head_gain[None, :],
        to_rows(factors), to_rows(moments), to_rows(weights),
    )
    held = pl.pallas_call(
        functools.partial(kernel, n, tp, heads),
        out_shape=(
            pltpu.VMEM((depth * per_row, LANES), jnp.bfloat16),
            pltpu.VMEM((depth * per_row, LANES), jnp.float32),
            pltpu.VMEM((rank_here * per_row, LANES), jnp.float32),
            pltpu.VMEM((2, LANES), jnp.float32),
        ),
        in_specs=[hbm] * len(args),
        out_specs=(vmem,) * 4,
        scratch_shapes=[
            pltpu.VMEM((length, depth), jnp.bfloat16),
            pltpu.VMEM((length, cols), jnp.bfloat16),
            pltpu.VMEM((length, cols), jnp.bfloat16),
            pltpu.VMEM((length, cols), jnp.bfloat16),
            pltpu.VMEM((length, cols), jnp.bfloat16),
            pltpu.SMEM((heads,), jnp.float32),
            pltpu.VMEM((1, head_gain.shape[0]), jnp.float32),
            pltpu.VMEM((deep * 2 * rank // LANES, LANES), jnp.bfloat16),
            pltpu.VMEM((rank_here * per_row, LANES), jnp.float32),
            pltpu.VMEM((deep * per_row, LANES), jnp.float32),
            pltpu.VMEM((depth, 2 * rank), jnp.bfloat16),
            pltpu.VMEM((n, 2, rank_here, cols), wire),
            pltpu.VMEM((deep * 2 * rank // LANES, LANES), jnp.float32),
            pltpu.VMEM((length, cols), jnp.bfloat16),
            pltpu.VMEM((length, cols), jnp.bfloat16),
            pltpu.VMEM((n, 2, rank_here, cols), wire),
            pltpu.VMEM((n, 2, rank_here, cols), wire),
            pltpu.VMEM((4, 2, rank_here, cols), wire),
            pltpu.VMEM((4, 2, rank_here, cols), wire),
            pltpu.VMEM((tp, 2, LANES), jnp.float32),
            dma((len(args),)),
            *(
                (
                    dma((1,)), dma((n,)), dma((1,)), dma((n, 3)),
                    dma((3,)), dma((n, CHUNKS)), dma((1,)), dma((n,)), dma((2,)), dma((n,)),
                )
                if n == 8
                else (dma((n,)), dma((n,)), dma((1,)), dma((1,)), dma((n,)), dma((n,)), dma((n,)), dma((n,)), dma((n,)), dma((n,)))
            ),
            dma((tp,)), dma((tp,)),
        ],
        compiler_params=pltpu.CompilerParams(
            collective_id=0, has_side_effects=True, vmem_limit_bytes=36 * 1024 * 1024
        ),
    )(*(pltpu.with_memory_space_constraint(arg, pltpu.HBM) for arg in args))
    out_hbm = pl.BlockSpec(memory_space=pltpu.HBM)
    step, new_moments, copies = pl.pallas_call(
        functools.partial(finish, n, rank * cols * tp),
        out_shape=(
            jax.ShapeDtypeStruct((deep * per_row, LANES), jnp.float32),
            jax.ShapeDtypeStruct((rank_here * per_row, LANES), jnp.float32),
            jax.ShapeDtypeStruct((depth * per_row, LANES), jnp.bfloat16),
        ),
        in_specs=[vmem] * 4,
        out_specs=(out_hbm,) * 3,
        scratch_shapes=[
            pltpu.VMEM((deep * per_row, LANES), jnp.float32),
            pltpu.VMEM((depth * per_row, LANES), jnp.bfloat16),
            dma((18,)),
        ],
        compiler_params=pltpu.CompilerParams(vmem_limit_bytes=16 * 1024 * 1024),
    )(*held)
    return from_rows(step, deep), from_rows(new_moments, rank_here), from_rows(copies, depth)


def solution(mesh):
    placed = (
        P("fs", None),
        P("fs", "tp"),
        P("fs", "tp"),
        P("fs", "tp"),
        P("fs", "tp"),
        P("tp"),
        P(),
        P("fs", None, None),
        P("fs", None, "tp"),
        P("fs", None, "tp"),
    )
    return jax.shard_map(
        functools.partial(per_device, mesh.shape["fs"], mesh.shape["tp"]),
        mesh=mesh,
        in_specs=placed,
        out_specs=(P("fs", None, "tp"), P("fs", None, "tp"), P(None, None, "tp")),
        check_vma=False,
    )
```

```python
import functools

import jax
import jax.numpy as jnp
from jax import lax
from jax.experimental import pallas as pl
from jax.experimental.pallas import tpu as pltpu
from jax.sharding import PartitionSpec as P

EPS = 0.05
BETA = 0.9
RATE_BASE = 0.5
MESH = pl.DeviceIdType.MESH
LANES = 128
CHUNKS = 8
WIDE = 2
SCHEDULE = [
    ("begin", "f"), ("own",), ("w", 0, 0, 19, 4), ("small", "f", (0,)), ("small", "f", (3,)), ("small", "f", (1,)),
    ("head", 0), ("w", 0, 2, 13, 4), ("small", "f", (2,)), ("head", 1), ("small", "f", (4,)), ("w", 0, 2, 14, 2),
    ("small", "f", (6,)), ("w", 2, 0, 17, 19), ("small", "f", (5,)), ("w", 4, 4, 7, 2), ("head", 2), ("head", 3),
    ("spread",), ("w", 3, 1, 16, 16), ("project",), ("pb",), ("w", 5, 10, 9, 4), ("w", 1, 1, 15, 6), ("pd", (0,), ()),
    ("pd", (1,), ()), ("w", 9, 1, 17, 5), ("w", 7, 4, 16, 5), ("w", 15, 5, 16, 19), ("pd", (2,), ()),
    ("pd", (3,), (0,)), ("pd", (4,), ()), ("w", 5, 3, 16, 1), ("w", 10, 0, 13, 3), ("w", 5, 3, 15, 1),
    ("pd", (5,), (1,)), ("pd", (6,), ()), ("w", 8, 0, 35, 12), ("pd", (7,), ()), ("w", 7, 1, 32, 13), ("pxs",),
    ("w", 14, 1, 35, 14), ("w", 3, 5, 39, 25), ("w", 14, 1, 36, 13), ("w", 11, 1, 35, 13), ("pd", (8,), ()),
    ("pd", (9,), ()), ("pt",), ("w", 1, 1, 40, 27), ("momentum",), ("begin", "n"), ("w", 24, 2, 15, 58),
    ("w", 24, 2, 16, 58), ("small", "n", (3,)), ("w", 23, 1, 15, 55), ("w", 24, 9, 55, 52), ("w", 22, 2, 55, 59),
    ("small", "n", (2,)), ("small", "n", (1,)), ("small", "n", (0,)), ("w", 25, 1, 0, 51), ("small", "n", (5,)),
    ("w", 26, 3, 18, 47), ("small", "n", (6,)), ("w", 26, 5, 18, 46), ("small", "n", (4,)), ("squares",),
    ("w", 24, 4, 17, 45), ("lows", 0), ("lows", 1), ("lows", 2), ("lows", 3), ("lows", 4), ("lows", 5),
    ("w", 29, 3, 59, 69), ("lows", 6), ("lows", 7), ("totals",), ("all", 43, 34, 17),
]


def split(ref, t, tiles, count):
    return ref[pl.ds(t % tiles * 2 + t // tiles, count, stride=2 * tiles), :]


def head_step(head, q_ref, k_ref, v_ref, c_ref, mix_ref, gain_ref, dq_ref, dv_ref):
    length = q_ref.shape[0]
    width = gain_ref.shape[1]
    half = width // 2
    factor = half ** (-0.5)
    cols = slice(head * width, (head + 1) * width)
    query, key, value = q_ref[:, cols], k_ref[:, cols], v_ref[:, cols]
    lane = lax.broadcasted_iota(jnp.int32, (length, width), 1)
    zero = jnp.zeros_like(key)
    key0 = jnp.where(lane < half, key, zero)
    key1 = jnp.where(lane < half, zero, key)
    row = lax.broadcasted_iota(jnp.int32, (length, length), 0)
    col = lax.broadcasted_iota(jnp.int32, (length, length), 1)
    causal = col <= row
    mix = mix_ref[head]
    nt = (((1,), (1,)), ((), ()))
    tn = (((0,), (0,)), ((), ()))

    def probs(rows):
        scores = lax.dot_general(query, rows, nt, preferred_element_type=jnp.float32) * factor
        scores = jnp.where(causal, scores, -jnp.inf)
        expo = jnp.exp(scores - jnp.max(scores, axis=-1, keepdims=True))
        return expo * (1.0 / jnp.sum(expo, axis=-1, keepdims=True))

    first, second = probs(key0), probs(key1)
    mixed = (first - mix * second).astype(jnp.bfloat16)
    output = jnp.dot(mixed, value, preferred_element_type=jnp.float32)
    inverse = lax.rsqrt(jnp.mean(output * output, axis=-1, keepdims=True) + EPS)
    scaled = gain_ref[...] * c_ref[:, cols].astype(jnp.float32)
    d_out = inverse * scaled - output * (inverse * inverse * inverse) * jnp.mean(
        output * scaled, axis=-1, keepdims=True
    )
    d_out = d_out.astype(jnp.bfloat16)
    dv_ref[:, cols] = lax.dot_general(mixed, d_out, tn, preferred_element_type=jnp.float32).astype(jnp.bfloat16)
    d_mix = lax.dot_general(d_out, value, nt, preferred_element_type=jnp.float32)
    d_first = first * (d_mix - jnp.sum(first * d_mix, axis=-1, keepdims=True))
    d_second = -mix * second * (d_mix - jnp.sum(second * d_mix, axis=-1, keepdims=True))
    d_query = jnp.dot(d_first.astype(jnp.bfloat16), key0, preferred_element_type=jnp.float32)
    d_query += jnp.dot(d_second.astype(jnp.bfloat16), key1, preferred_element_type=jnp.float32)
    dq_ref[:, cols] = (d_query * factor).astype(jnp.bfloat16)


class Lists:
    def __init__(self):
        def source(k, order):
            return [(k, True, c) for c in order] + [(k, False, c) for c in range(WIDE)]

        order = list(range(WIDE, CHUNKS)) + list(range(WIDE))
        mirror = lambda entries: [(3 - k, same, c) for k, same, c in entries]
        first = source(0, order)
        inner = source(1, order)
        self.up = {0: first, 1: self.merge(inner, first)}
        far = mirror(self.up[1])
        self.down = {0: [], 1: self.merge(inner, far)}
        self.from_up = {0: self.down[1], 1: far}
        self.from_down = {0: [], 1: first}
        own = lambda q: [(q, True, c) for c in range(CHUNKS)]
        narrow = lambda entries: [e for e in entries if e[1] and e[2] >= WIDE]
        self.cross = {
            0: own(0) + narrow(self.from_up[0]),
            1: own(1) + self.weave(narrow(self.from_down[1]), narrow(self.from_up[1])),
        }
        self.from_cross = {q: [(k, not same, c) for k, same, c in self.cross[q]] for q in (0, 1)}

    @staticmethod
    def merge(own, passed):
        return own + passed

    @staticmethod
    def weave(a, b):
        out = []
        for i in range(max(len(a), len(b))):
            out += a[i : i + 1] + b[i : i + 1]
        return out


class Weights:
    def __init__(self, lists, q):
        self.q = q
        self.out = {"up": list(lists.up[q]), "down": list(lists.down[q]), "cross": list(lists.cross[q])}
        self.into = {
            "cross": list(lists.from_cross[q]), "down": list(lists.from_down[q]), "up": list(lists.from_up[q]),
        }
        self.have = {(q, True, c) for c in range(CHUNKS)}
        self.got = {way: 0 for way in self.into}
        self.put = {way: 0 for way in self.out}

    def push(self, along, across):
        moves = []
        for way, goal in (("up", along), ("down", along), ("cross", across)):
            while self.put[way] < min(len(self.out[way]), goal):
                entry = self.out[way][self.put[way]]
                if entry not in self.have:
                    break
                moves.append(("send", way, entry))
                self.put[way] += 1
        return moves

    def take(self, along, across, push_along, push_across):
        moves = self.push(push_along, push_across)
        goals = {"cross": across, "down": along, "up": along}
        for count in range(1, max(along, across) + 1):
            for way, goal in goals.items():
                if self.got[way] < min(len(self.into[way]), goal, count):
                    entry = self.into[way][self.got[way]]
                    moves.append(("wait", way, entry))
                    self.have.add(entry)
                    self.got[way] += 1
                    moves += self.push(push_along, push_across)
        return moves

    def done(self):
        return all(self.got[w] == len(self.into[w]) for w in self.into) and all(
            self.put[w] == len(self.out[w]) for w in self.out
        )


def kernel(
    n, tp, heads,
    x_hbm, q_hbm, k_hbm, v_hbm, c_hbm, mix_hbm, gain_hbm, f_hbm, mom_hbm, w_hbm,
    wall, low, nm_ref, tot_ref,
    x_ref, q_ref, k_ref, v_ref, c_ref, mix_ref, gain_ref, f_ref, mom_ref, w_ref,
    fall, nmall, fwide, dq, dv, psend, precv, pin, pmid, xsend, xrecv, ptot, sums,
    l_sem, f_send, f_recv, s_send, s_recv, w_send, w_recv, n_send, n_recv, p_send, p_recv, t_send, t_recv,
):
    me = lax.axis_index("fs")
    mt = lax.axis_index("tp")
    depth = fall.shape[0]
    deep = depth // n
    rank = fall.shape[1] // 2
    rank_here = rank // n
    cols = dq.shape[1]
    tiles_f, tiles_w = rank // LANES, cols // LANES
    per_row = 2 * tiles_w

    local = {}
    for i, (name, src, dst) in enumerate((
        ("f", f_hbm, f_ref), ("w", w_hbm, w_ref), ("gain", gain_hbm, gain_ref), ("mix", mix_hbm, mix_ref),
        ("q", q_hbm, q_ref), ("k", k_hbm, k_ref), ("v", v_hbm, v_ref), ("c", c_hbm, c_ref),
        ("x", x_hbm, x_ref), ("mom", mom_hbm, mom_ref),
    )):
        local[name] = pltpu.make_async_copy(src, dst, l_sem.at[i])
        local[name].start()

    barrier = pltpu.get_barrier_semaphore()
    for hop in range(1, n):
        pl.semaphore_signal(barrier, inc=1, device_id={"fs": (me + hop) % n}, device_id_type=MESH)
    for hop in range(1, tp):
        pl.semaphore_signal(barrier, inc=1, device_id={"tp": (mt + hop) % tp}, device_id_type=MESH)

    local["f"].wait()
    fwide[...] = f_ref[...].astype(jnp.float32)
    here = pl.ds(pl.multiple_of(me * deep, deep), deep)
    for t in range(2 * tiles_f):
        fall[here, t * LANES : (t + 1) * LANES] = split(fwide, t, tiles_f, deep).astype(jnp.bfloat16)

    def own_weights():
        local["w"].wait()
        wall[pl.ds(pl.multiple_of(me * deep * per_row, 16), deep * per_row), :] = w_ref[...].astype(jnp.bfloat16)

    def head(i):
        if i == 0:
            for name in ("gain", "mix", "q", "k", "v", "c"):
                local[name].wait()
        head_step(i, q_ref, k_ref, v_ref, c_ref, mix_ref, gain_ref, dq, dv)

    def remote(src, send, recv, axis, target):
        return pltpu.make_async_remote_copy(
            src_ref=src, dst_ref=src, send_sem=send, recv_sem=recv, device_id={axis: target}, device_id_type=MESH
        )

    def project():
        local["x"].wait()
        for m, cot in enumerate((dq, dv)):
            reduced = jnp.dot(
                x_ref[...], fall[:, m * rank : (m + 1) * rank], preferred_element_type=jnp.float32
            ).astype(jnp.bfloat16)
            partial = lax.dot_general(
                reduced, cot[...], (((0,), (0,)), ((), ())), preferred_element_type=jnp.float32
            )
            for j in range(n):
                psend[j, m] = partial[j * rank_here : (j + 1) * rank_here].astype(psend.dtype)

    def p_copy(hop):
        peer = (me + hop) % n
        return pltpu.make_async_remote_copy(
            src_ref=psend.at[peer], dst_ref=precv.at[hop], send_sem=p_send.at[hop], recv_sem=p_recv.at[hop],
            device_id={"fs": peer}, device_id_type=MESH,
        )

    def momentum(total):
        local["mom"].wait()
        length = x_ref.shape[0]
        for t in range(2 * tiles_w):
            m, lanes = t // tiles_w, slice(t % tiles_w * LANES, (t % tiles_w + 1) * LANES)
            moments = BETA * split(mom_ref, t, tiles_w, rank_here)
            moments += total[m, :, lanes] * (length * n) ** (-0.5)
            nm_ref[pl.ds(t % tiles_w * 2 + m, rank_here, stride=per_row), :] = moments
            nmall[me, m, :, lanes] = moments.astype(nmall.dtype)

    def t_copy(hop):
        return pltpu.make_async_remote_copy(
            src_ref=sums.at[0], dst_ref=sums.at[hop], send_sem=t_send.at[hop], recv_sem=t_recv.at[hop],
            device_id={"tp": (mt + hop) % tp}, device_id_type=MESH,
        )

    def squares():
        everything = nmall[...].astype(jnp.float32)
        parts = jnp.sum(jnp.sum(everything * everything, axis=0), axis=1)
        sums[0] = jnp.sum(parts, axis=1, keepdims=True) + jnp.zeros((2, LANES), jnp.float32)
        for hop in range(1, tp):
            t_copy(hop).start()

    def totals():
        result = sums[0]
        for hop in range(1, tp):
            t_copy(hop).wait_recv()
            result += sums[hop]
        tot_ref[...] = result

    def lows(start, count):
        for m in range(2):
            block = nmall[:, m].reshape(rank, cols).astype(jnp.bfloat16)
            product = jnp.dot(
                fall[start : start + count, m * rank : (m + 1) * rank], block, preferred_element_type=jnp.float32
            )
            for t in range(tiles_w):
                low[pl.ds(start * per_row + 2 * t + m, count, stride=per_row), :] = (
                    product[:, t * LANES : (t + 1) * LANES]
                )

    def weights(index, chunk, chunks):
        size = deep // chunks * per_row
        return wall.at[pl.ds(pl.multiple_of(index * deep * per_row + chunk * size, 16), size)]

    quarter = 2 * rank // tp
    if n == 8 and tp == 4 and quarter % LANES == 0 and deep % (2 * CHUNKS) == 0:
        place, parity = me // 2, me % 2
        flip = place // 2
        side = jnp.where(flip == 0, place, 3 - place)
        lists = Lists()
        states = [Weights(lists, q) for q in (0, 1)]
        partner = me + 1 - 2 * parity
        far, near = (mt + 2) % tp, mt + 1 - 2 * (mt % 2)

        def index_of(k, same):
            return 2 * (k + flip * (3 - 2 * k)) + (parity if same else 1 - parity)

        def target(q, way):
            return partner if way == "cross" else index_of(q + 1 if way == "up" else q - 1, True)

        ways = {"up": 0, "down": 1, "cross": 2}

        def w_copy(q, way, entry):
            k, same, chunk = entry
            index = index_of(k, same)
            return remote(
                weights(index, chunk, CHUNKS), w_send.at[ways[way]], w_recv.at[index, chunk],
                "fs", target(q, way),
            )

        def run(q, moves):
            for kind, way, entry in moves:
                if kind == "send":
                    w_copy(q, way, entry).start()
                else:
                    w_copy(q, "cross", entry).wait_recv()

        def piece(index, which):
            return fall.at[
                pl.ds(pl.multiple_of(index * deep, deep), deep), pl.ds(pl.multiple_of(which * quarter, quarter), quarter)
            ]

        def others(q):
            return sorted((k for k in range(4) if k != q), key=lambda k: (abs(k - q), k))

        def small(kind, index, to):
            if kind == "f":
                return remote(piece(index, mt), f_send.at[0], f_recv.at[index], "fs", to)
            return remote(nmall.at[index], n_send.at[0], n_recv.at[index], "fs", to)

        def small_begin(kind, q):
            for i, k in enumerate(reversed(others(q))):
                small(kind, me, index_of(k, True)).start()
            small(kind, me, partner).start()

        def spread(index, which, to, way):
            return remote(piece(index, which), s_send.at[0], s_recv.at[index, way], "tp", to)

        def small_wait(kind, q, k, same):
            index = index_of(k, same)
            small(kind, index, partner).wait_recv()
            if same:
                small(kind, index, partner).start()
            if kind == "f":
                spread(index, mt, far, 0).start()
                spread(index, mt, near, 1).start()

        def pieces(q):
            return [(q, False)] + [(k, True) for k in others(q)] + [(k, False) for k in others(q)]

        def place_of(k):
            return k + flip * (3 - 2 * k)

        def p_items(q):
            if q == 0:
                return [("down", 0, False), ("down", 0, True)]
            return [
                ("up", 3, False), ("up", 3, True), ("up", 2, False), ("down", 0, False), ("up", 2, True),
                ("down", 0, True), ("up", 1, False), ("down", 1, False), ("up", 1, True), ("down", 1, True),
            ]

        def p_slot(way, k, same):
            w = 0 if way == "up" else 1
            return (w + flip * (1 - 2 * w)) * 8 + place_of(k) * 2 + (0 if same else 1)

        def p_hop(q, way, k, same, src):
            slot = p_slot(way, k, same)
            to = min(max(q + (1 if way == "up" else -1), 0), 3)
            return pltpu.make_async_remote_copy(
                src_ref=src, dst_ref=pin.at[slot], send_sem=p_send.at[0], recv_sem=p_recv.at[slot],
                device_id={"fs": index_of(to, True)}, device_id_type=MESH,
            )

        def p_pass(q, way, k, same):
            slot = p_slot(way, k, same)
            p_hop(1, way, k, same, pin.at[slot]).wait_recv()
            if k != q:
                pmid[slot] = (
                    psend[index_of(k, same)].astype(jnp.float32) + pin[slot].astype(jnp.float32)
                ).astype(pmid.dtype)
                p_hop(q, way, k, same, pmid.at[slot]).start()

        def p_sum(q, same):
            total = psend[me if same else partner].astype(jnp.float32)
            for way, k, parity_same in p_items(q):
                if k == q and parity_same == same:
                    total += pin[p_slot(way, k, same)].astype(jnp.float32)
            return total

        def p_cross():
            return pltpu.make_async_remote_copy(
                src_ref=xsend, dst_ref=xrecv, send_sem=p_send.at[1], recv_sem=p_recv.at[16],
                device_id={"fs": partner}, device_id_type=MESH,
            )

        def gathered():
            p_cross().wait_recv()
            return ptot[...] + xrecv[...].astype(jnp.float32)

        def segment(tokens):
            for q in (0, 1):

                @pl.when(side == q)
                def _(q=q):
                    for token in tokens:
                        kind, *rest = token
                        if kind == "w":
                            run(q, states[q].take(*rest))
                        elif kind == "begin":
                            small_begin(rest[0], q)
                        elif kind == "pb" and q == 0:
                            for k in (3, 2, 1):
                                for same in (False, True):
                                    p_hop(q, "up", k, same, psend.at[index_of(k, same)]).start()
                        elif kind == "pd":
                            for i in rest[1 - q]:
                                p_pass(q, *p_items(q)[i])
                        elif kind == "pxs":
                            xsend[...] = p_sum(q, False).astype(xsend.dtype)
                            p_cross().start()
                        elif kind == "pt":
                            ptot[...] = p_sum(q, True)
                        elif kind == "small":
                            for i in rest[1]:
                                small_wait(rest[0], q, *pieces(q)[i])
                        elif kind == "all":
                            along, across, ahead = rest
                            while not states[q].done():
                                run(q, states[q].take(along, across, along + ahead, across + ahead))
                                along, across = along + 1, across + 1
                        elif kind == "spread":
                            for k, same in pieces(q):
                                index = index_of(k, same)
                                spread(index, far, far, 0).wait_recv()
                                spread(index, far, near, 2).start()
                            for k, same in pieces(q):
                                index = index_of(k, same)
                                spread(index, near, near, 1).wait_recv()
                                spread(index, (near + 2) % tp, near, 2).wait_recv()
                        elif kind == "sent":
                            for way in ways:
                                if states[q].out[way]:
                                    all_sent(wall, w_send.at[ways[way]], len(states[q].out[way]), CHUNKS)

        def all_sent(whole, sem, count, per_block):
            rows = whole.shape[0] // n // per_block * count
            part = whole.at[pl.ds(0, rows)]
            remote(part, sem, sem, "fs", partner).wait_send()

        def rest_sent():
            all_sent(fall, f_send.at[0], 7, tp)
            all_sent(fall, s_send.at[0], 21, tp)
            all_sent(nmall, n_send.at[0], 7, 1)
            remote(pmid.at[pl.ds(0, 6)], p_send.at[0], p_send.at[0], "fs", partner).wait_send()
            p_cross().wait_send()

        computes = {
            "own": own_weights, "project": project, "squares": squares, "totals": totals, "momentum": lambda: momentum(gathered()),
            "lows": lambda j: lows(j * deep, deep),
        }
        pl.semaphore_wait(barrier, n - 1 + tp - 1)
        for token in SCHEDULE:
            if token[0] == "head":
                for i in range(token[1], heads if token[1] == 3 else token[1] + 1):
                    head(i)
            elif token[0] in computes:
                computes[token[0]](*token[1:])
            else:
                segment([token])
        segment([("sent",)])
        rest_sent()
    else:
        own_weights()
        for i in range(heads):
            head(i)
        pl.semaphore_wait(barrier, n - 1 + tp - 1)

        def block(kind, index, hop):
            if kind == "f":
                return remote(
                    fall.at[pl.ds(pl.multiple_of(index * deep, 8), deep)], f_send.at[hop], f_recv.at[index],
                    "fs", (me + hop) % n,
                )
            if kind == "w":
                return remote(weights(index, 0, 1), w_send.at[hop], w_recv.at[index], "fs", (me + hop) % n)
            return remote(nmall.at[index], n_send.at[hop], n_recv.at[index], "fs", (me + hop) % n)

        def each(action):
            def step(hop, carry):
                action(hop)
                return carry

            lax.fori_loop(1, n, step, 0)

        each(lambda hop: block("f", me, hop).start())
        each(lambda hop: block("w", me, hop).start())
        each(lambda hop: block("f", (me + hop) % n, hop).wait_recv())
        project()
        each(lambda hop: p_copy(hop).start())

        def add(hop, total):
            p_copy(hop).wait_recv()
            return total + precv[hop].astype(jnp.float32)

        momentum(lax.fori_loop(1, n, add, psend[me].astype(jnp.float32)))
        each(lambda hop: block("n", me, hop).start())
        each(lambda hop: block("n", (me + hop) % n, hop).wait_recv())
        squares()
        for start in range(0, depth, 256):
            lows(start, min(256, depth - start))
        totals()
        each(lambda hop: block("w", (me + hop) % n, hop).wait_recv())
        for kind in ("f", "w", "n"):
            each(lambda hop, kind=kind: block(kind, me, hop).wait_send())
        each(lambda hop: p_copy(hop).wait_send())
    for hop in range(1, tp):
        t_copy(hop).wait_send()


def finish(n, entries, wall, low, nm_ref, tot_ref, step_hbm, nm_hbm, copies_hbm, step, copies, sems):
    me = lax.axis_index("fs")
    rows = low.shape[0]
    own = rows // n
    nm_copy = pltpu.make_async_copy(nm_ref, nm_hbm, sems.at[0])
    nm_copy.start()
    rate = RATE_BASE / jnp.sqrt(1.0 + tot_ref[...] / entries)
    count = min(rows // 16, 1024)
    odd = lax.broadcasted_iota(jnp.int32, (count, LANES), 0) % 2 == 1
    rates = jnp.where(odd, rate[1:2], rate[0:1])
    started = [nm_copy]
    for i in range(0, own, min(count, own)):
        size = min(count, own)
        start = pl.multiple_of(me * own + i, 8)
        step[i : i + size, :] = low[pl.ds(start, size), :] * rates[:size]
    started.append(pltpu.make_async_copy(step, step_hbm, sems.at[1]))
    started[-1].start()
    for i in range(rows // count):
        at = slice(i * count, (i + 1) * count)
        copies[at, :] = (wall[at, :].astype(jnp.float32) - low[at, :] * rates).astype(jnp.bfloat16)
        started.append(pltpu.make_async_copy(copies.at[at], copies_hbm.at[at], sems.at[2 + i]))
        started[-1].start()
    for copy in started:
        copy.wait()


def to_rows(array):
    rows, maps, cols = array.shape
    return array.reshape(rows, maps, cols // LANES, LANES).transpose(0, 2, 1, 3).reshape(-1, LANES)


def from_rows(array, rows):
    return (
        array.reshape(rows, -1, 2, LANES).transpose(0, 2, 1, 3).reshape(rows, 2, -1)
    )


def per_device(
    n, tp, inputs, queries, keys, values, head_cot, mixing, head_gain, factors, moments, weights
):
    length, depth = inputs.shape
    heads = mixing.shape[0]
    deep, _, rank = factors.shape
    rank_here, _, cols = moments.shape
    wire = jnp.bfloat16 if rank_here % 16 == 0 else jnp.float32
    per_row = 2 * cols // LANES
    hbm = pl.BlockSpec(memory_space=pltpu.HBM)
    vmem = pl.BlockSpec(memory_space=pltpu.VMEM)
    dma = pltpu.SemaphoreType.DMA
    args = (
        inputs, queries, keys, values, head_cot, mixing, head_gain[None, :],
        to_rows(factors), to_rows(moments), to_rows(weights),
    )
    semaphores = [
            dma((len(args),)),
            *(
                (
                    dma((1,)), dma((n,)), dma((1,)), dma((n, 3)),
                    dma((3,)), dma((n, CHUNKS)), dma((1,)), dma((n,)), dma((2,)), dma((17,)),
                )
                if n == 8
                else (dma((n,)), dma((n,)), dma((1,)), dma((1,)), dma((n,)), dma((n,)), dma((n,)), dma((n,)), dma((n,)), dma((n,)))
            ),
            dma((tp,)), dma((tp,)),
    ]

    def scoped(*refs):
        pl.run_scoped(lambda *sems: kernel(n, tp, heads, *refs, *sems), *semaphores)

    held = pl.pallas_call(
        scoped,
        out_shape=(
            pltpu.VMEM((depth * per_row, LANES), jnp.bfloat16),
            pltpu.VMEM((depth * per_row, LANES), jnp.float32),
            pltpu.VMEM((rank_here * per_row, LANES), jnp.float32),
            pltpu.VMEM((2, LANES), jnp.float32),
        ),
        in_specs=[hbm] * len(args),
        out_specs=(vmem,) * 4,
        scratch_shapes=[
            pltpu.VMEM((length, depth), jnp.bfloat16),
            pltpu.VMEM((length, cols), jnp.bfloat16),
            pltpu.VMEM((length, cols), jnp.bfloat16),
            pltpu.VMEM((length, cols), jnp.bfloat16),
            pltpu.VMEM((length, cols), jnp.bfloat16),
            pltpu.SMEM((heads,), jnp.float32),
            pltpu.VMEM((1, head_gain.shape[0]), jnp.float32),
            pltpu.VMEM((deep * 2 * rank // LANES, LANES), jnp.bfloat16),
            pltpu.VMEM((rank_here * per_row, LANES), jnp.float32),
            pltpu.VMEM((deep * per_row, LANES), jnp.float32),
            pltpu.VMEM((depth, 2 * rank), jnp.bfloat16),
            pltpu.VMEM((n, 2, rank_here, cols), wire),
            pltpu.VMEM((deep * 2 * rank // LANES, LANES), jnp.float32),
            pltpu.VMEM((length, cols), jnp.bfloat16),
            pltpu.VMEM((length, cols), jnp.bfloat16),
            pltpu.VMEM((n, 2, rank_here, cols), wire),
            pltpu.VMEM((n, 2, rank_here, cols), wire),
            pltpu.VMEM((16 if n == 8 else 1, 2, rank_here, cols), wire),
            pltpu.VMEM((16 if n == 8 else 1, 2, rank_here, cols), wire),
            pltpu.VMEM((2, rank_here, cols), wire),
            pltpu.VMEM((2, rank_here, cols), wire),
            pltpu.VMEM((2, rank_here, cols), jnp.float32),
            pltpu.VMEM((tp, 2, LANES), jnp.float32),
        ],
        compiler_params=pltpu.CompilerParams(
            collective_id=0, has_side_effects=True, vmem_limit_bytes=36 * 1024 * 1024
        ),
    )(*(pltpu.with_memory_space_constraint(arg, pltpu.HBM) for arg in args))
    out_hbm = pl.BlockSpec(memory_space=pltpu.HBM)
    step, new_moments, copies = pl.pallas_call(
        functools.partial(finish, n, rank * cols * tp),
        out_shape=(
            jax.ShapeDtypeStruct((deep * per_row, LANES), jnp.float32),
            jax.ShapeDtypeStruct((rank_here * per_row, LANES), jnp.float32),
            jax.ShapeDtypeStruct((depth * per_row, LANES), jnp.bfloat16),
        ),
        in_specs=[vmem] * 4,
        out_specs=(out_hbm,) * 3,
        scratch_shapes=[
            pltpu.VMEM((deep * per_row, LANES), jnp.float32),
            pltpu.VMEM((depth * per_row, LANES), jnp.bfloat16),
            dma((18,)),
        ],
        compiler_params=pltpu.CompilerParams(vmem_limit_bytes=16 * 1024 * 1024),
    )(*held)
    return from_rows(step, deep), from_rows(new_moments, rank_here), from_rows(copies, depth)


def solution(mesh):
    placed = (
        P("fs", None),
        P("fs", "tp"),
        P("fs", "tp"),
        P("fs", "tp"),
        P("fs", "tp"),
        P("tp"),
        P(),
        P("fs", None, None),
        P("fs", None, "tp"),
        P("fs", None, "tp"),
    )
    return jax.shard_map(
        functools.partial(per_device, mesh.shape["fs"], mesh.shape["tp"]),
        mesh=mesh,
        in_specs=placed,
        out_specs=(P("fs", None, "tp"), P("fs", None, "tp"), P(None, None, "tp")),
        check_vma=False,
    )
```

```python
import functools

import jax
import jax.numpy as jnp
from jax import lax
from jax.experimental import pallas as pl
from jax.experimental.pallas import tpu as pltpu
from jax.sharding import PartitionSpec as P

EPS = 0.05
BETA = 0.9
RATE_BASE = 0.5
MESH = pl.DeviceIdType.MESH
LANES = 128
CHUNKS = 16
WIDE = 3
SCHEDULE = [
    ("begin", "f"), ("own",), ("w", 0, 0, 93, 9), ("small", "f", (0,)), ("small", "f", (3,)), ("small", "f", (1,)),
    ("small", "f", (2,)), ("head", 0), ("w", 1, 0, 92, 4), ("w", 0, 0, 92, 4), ("w", 0, 0, 75, 10),
    ("w", 0, 2, 77, 14), ("w", 1, 2, 74, 16), ("head", 1), ("w", 2, 2, 77, 17), ("small", "f", (6,)), ("head", 2),
    ("w", 0, 9, 45, 67), ("small", "f", (4,)), ("head", 3), ("small", "f", (5,)), ("w", 7, 10, 42, 60),
    ("w", 9, 0, 52, 0), ("spread",), ("project",), ("w", 7, 5, 42, 57), ("pb",), ("pd", (0,), ()), ("pd", (1,), ()),
    ("w", 2, 2, 53, 59), ("w", 16, 6, 31, 53), ("w", 28, 7, 29, 44), ("pd", (2,), ()), ("pd", (3,), (0,)),
    ("w", 0, 11, 25, 24), ("pd", (4,), ()), ("pd", (5,), (1,)), ("w", 22, 33, 43, 46), ("pd", (6,), ()),
    ("pd", (7,), ()), ("pxs",), ("pd", (8,), ()), ("pd", (9,), ()), ("pt",), ("w", 24, 30, 35, 59),
    ("w", 22, 17, 63, 39), ("w", 23, 38, 64, 47), ("w", 16, 32, 55, 43), ("w", 19, 27, 65, 49), ("momentum",),
    ("begin", "n"), ("w", 46, 26, 33, 95), ("small", "n", (0,)), ("small", "n", (3,)), ("w", 19, 46, 71, 37),
    ("small", "n", (2,)), ("small", "n", (1,)), ("w", 51, 32, 20, 53), ("w", 52, 23, 24, 67), ("small", "n", (5,)),
    ("small", "n", (4,)), ("small", "n", (6,)), ("squares",), ("w", 41, 35, 22, 57), ("lows", 0), ("lows", 1),
    ("lows", 2), ("w", 39, 31, 41, 52), ("lows", 3), ("w", 53, 30, 24, 52), ("w", 54, 23, 21, 48), ("lows", 4),
    ("lows", 5), ("w", 55, 23, 21, 48), ("lows", 6), ("lows", 7), ("totals",), ("all", 117, 122, 81),
]


def split(ref, t, tiles, count):
    return ref[pl.ds(t % tiles * 2 + t // tiles, count, stride=2 * tiles), :]


def head_step(head, q_ref, k_ref, v_ref, c_ref, mix_ref, gain_ref, dq_ref, dv_ref):
    length = q_ref.shape[0]
    width = gain_ref.shape[1]
    half = width // 2
    factor = half ** (-0.5)
    cols = slice(head * width, (head + 1) * width)
    query, key, value = q_ref[:, cols], k_ref[:, cols], v_ref[:, cols]
    lane = lax.broadcasted_iota(jnp.int32, (length, width), 1)
    zero = jnp.zeros_like(key)
    key0 = jnp.where(lane < half, key, zero)
    key1 = jnp.where(lane < half, zero, key)
    row = lax.broadcasted_iota(jnp.int32, (length, length), 0)
    col = lax.broadcasted_iota(jnp.int32, (length, length), 1)
    causal = col <= row
    mix = mix_ref[head]
    nt = (((1,), (1,)), ((), ()))
    tn = (((0,), (0,)), ((), ()))

    def probs(rows):
        scores = lax.dot_general(query, rows, nt, preferred_element_type=jnp.float32) * factor
        scores = jnp.where(causal, scores, -jnp.inf)
        expo = jnp.exp(scores - jnp.max(scores, axis=-1, keepdims=True))
        return expo * (1.0 / jnp.sum(expo, axis=-1, keepdims=True))

    first, second = probs(key0), probs(key1)
    mixed = (first - mix * second).astype(jnp.bfloat16)
    output = jnp.dot(mixed, value, preferred_element_type=jnp.float32)
    inverse = lax.rsqrt(jnp.mean(output * output, axis=-1, keepdims=True) + EPS)
    scaled = gain_ref[...] * c_ref[:, cols].astype(jnp.float32)
    d_out = inverse * scaled - output * (inverse * inverse * inverse) * jnp.mean(
        output * scaled, axis=-1, keepdims=True
    )
    d_out = d_out.astype(jnp.bfloat16)
    dv_ref[:, cols] = lax.dot_general(mixed, d_out, tn, preferred_element_type=jnp.float32).astype(jnp.bfloat16)
    d_mix = lax.dot_general(d_out, value, nt, preferred_element_type=jnp.float32)
    d_first = first * (d_mix - jnp.sum(first * d_mix, axis=-1, keepdims=True))
    d_second = -mix * second * (d_mix - jnp.sum(second * d_mix, axis=-1, keepdims=True))
    d_query = jnp.dot(d_first.astype(jnp.bfloat16), key0, preferred_element_type=jnp.float32)
    d_query += jnp.dot(d_second.astype(jnp.bfloat16), key1, preferred_element_type=jnp.float32)
    dq_ref[:, cols] = (d_query * factor).astype(jnp.bfloat16)


class Lists:
    def __init__(self):
        def source(k, order):
            return [(k, True, c) for c in order] + [(k, False, c) for c in range(WIDE)]

        order = list(range(WIDE, CHUNKS)) + list(range(WIDE))
        mirror = lambda entries: [(3 - k, same, c) for k, same, c in entries]
        first = source(0, order)
        inner = source(1, order)
        self.up = {0: first, 1: self.merge(inner, first)}
        far = mirror(self.up[1])
        self.down = {0: [], 1: self.merge(inner, far)}
        self.from_up = {0: self.down[1], 1: far}
        self.from_down = {0: [], 1: first}
        own = lambda q: [(q, True, c) for c in range(CHUNKS)]
        narrow = lambda entries: [e for e in entries if e[1] and e[2] >= WIDE]
        self.cross = {
            0: own(0) + narrow(self.from_up[0]),
            1: own(1) + self.weave(narrow(self.from_down[1]), narrow(self.from_up[1])),
        }
        self.from_cross = {q: [(k, not same, c) for k, same, c in self.cross[q]] for q in (0, 1)}

    @staticmethod
    def merge(own, passed):
        return own + passed

    @staticmethod
    def weave(a, b):
        out = []
        for i in range(max(len(a), len(b))):
            out += a[i : i + 1] + b[i : i + 1]
        return out


class Weights:
    def __init__(self, lists, q):
        self.q = q
        self.out = {"up": list(lists.up[q]), "down": list(lists.down[q]), "cross": list(lists.cross[q])}
        self.into = {
            "cross": list(lists.from_cross[q]), "down": list(lists.from_down[q]), "up": list(lists.from_up[q]),
        }
        self.have = {(q, True, c) for c in range(CHUNKS)}
        self.got = {way: 0 for way in self.into}
        self.put = {way: 0 for way in self.out}

    def push(self, along, across):
        moves = []
        for way, goal in (("up", along), ("down", along), ("cross", across)):
            while self.put[way] < min(len(self.out[way]), goal):
                entry = self.out[way][self.put[way]]
                if entry not in self.have:
                    break
                moves.append(("send", way, entry))
                self.put[way] += 1
        return moves

    def take(self, along, across, push_along, push_across):
        moves = self.push(push_along, push_across)
        goals = {"cross": across, "down": along, "up": along}
        for count in range(1, max(along, across) + 1):
            for way, goal in goals.items():
                if self.got[way] < min(len(self.into[way]), goal, count):
                    entry = self.into[way][self.got[way]]
                    moves.append(("wait", way, entry))
                    self.have.add(entry)
                    self.got[way] += 1
                    moves += self.push(push_along, push_across)
        return moves

    def done(self):
        return all(self.got[w] == len(self.into[w]) for w in self.into) and all(
            self.put[w] == len(self.out[w]) for w in self.out
        )


def kernel(
    n, tp, heads,
    x_hbm, q_hbm, k_hbm, v_hbm, c_hbm, mix_hbm, gain_hbm, f_hbm, mom_hbm, w_hbm,
    wall, low, nm_ref, tot_ref,
    x_ref, q_ref, k_ref, v_ref, c_ref, mix_ref, gain_ref, f_ref, mom_ref, w_ref,
    fall, nmall, fwide, dq, dv, psend, precv, pin, pmid, xsend, xrecv, ptot, sums,
    l_sem, f_send, f_recv, s_send, s_recv, w_send, w_recv, n_send, n_recv, p_send, p_recv, t_send, t_recv,
):
    me = lax.axis_index("fs")
    mt = lax.axis_index("tp")
    depth = fall.shape[0]
    deep = depth // n
    rank = fall.shape[1] // 2
    rank_here = rank // n
    cols = dq.shape[1]
    tiles_f, tiles_w = rank // LANES, cols // LANES
    per_row = 2 * tiles_w

    local = {}
    for i, (name, src, dst) in enumerate((
        ("f", f_hbm, f_ref), ("w", w_hbm, w_ref), ("gain", gain_hbm, gain_ref), ("mix", mix_hbm, mix_ref),
        ("q", q_hbm, q_ref), ("k", k_hbm, k_ref), ("v", v_hbm, v_ref), ("c", c_hbm, c_ref),
        ("x", x_hbm, x_ref), ("mom", mom_hbm, mom_ref),
    )):
        local[name] = pltpu.make_async_copy(src, dst, l_sem.at[i])
        local[name].start()

    barrier = pltpu.get_barrier_semaphore()
    for hop in range(1, n):
        pl.semaphore_signal(barrier, inc=1, device_id={"fs": (me + hop) % n}, device_id_type=MESH)
    for hop in range(1, tp):
        pl.semaphore_signal(barrier, inc=1, device_id={"tp": (mt + hop) % tp}, device_id_type=MESH)

    local["f"].wait()
    fwide[...] = f_ref[...].astype(jnp.float32)
    here = pl.ds(pl.multiple_of(me * deep, deep), deep)
    for t in range(2 * tiles_f):
        fall[here, t * LANES : (t + 1) * LANES] = split(fwide, t, tiles_f, deep).astype(jnp.bfloat16)

    def own_weights():
        local["w"].wait()
        wall[pl.ds(pl.multiple_of(me * deep * per_row, 16), deep * per_row), :] = w_ref[...].astype(jnp.bfloat16)

    def head(i):
        if i == 0:
            for name in ("gain", "mix", "q", "k", "v", "c"):
                local[name].wait()
        head_step(i, q_ref, k_ref, v_ref, c_ref, mix_ref, gain_ref, dq, dv)

    def remote(src, send, recv, axis, target):
        return pltpu.make_async_remote_copy(
            src_ref=src, dst_ref=src, send_sem=send, recv_sem=recv, device_id={axis: target}, device_id_type=MESH
        )

    def project():
        local["x"].wait()
        for m, cot in enumerate((dq, dv)):
            reduced = jnp.dot(
                x_ref[...], fall[:, m * rank : (m + 1) * rank], preferred_element_type=jnp.float32
            ).astype(jnp.bfloat16)
            partial = lax.dot_general(
                reduced, cot[...], (((0,), (0,)), ((), ())), preferred_element_type=jnp.float32
            )
            for j in range(n):
                psend[j, m] = partial[j * rank_here : (j + 1) * rank_here].astype(psend.dtype)

    def p_copy(hop):
        peer = (me + hop) % n
        return pltpu.make_async_remote_copy(
            src_ref=psend.at[peer], dst_ref=precv.at[hop], send_sem=p_send.at[hop], recv_sem=p_recv.at[hop],
            device_id={"fs": peer}, device_id_type=MESH,
        )

    def momentum(total):
        local["mom"].wait()
        length = x_ref.shape[0]
        for t in range(2 * tiles_w):
            m, lanes = t // tiles_w, slice(t % tiles_w * LANES, (t % tiles_w + 1) * LANES)
            moments = BETA * split(mom_ref, t, tiles_w, rank_here)
            moments += total[m, :, lanes] * (length * n) ** (-0.5)
            nm_ref[pl.ds(t % tiles_w * 2 + m, rank_here, stride=per_row), :] = moments
            nmall[me, m, :, lanes] = moments.astype(nmall.dtype)

    def t_copy(hop):
        return pltpu.make_async_remote_copy(
            src_ref=sums.at[0], dst_ref=sums.at[hop], send_sem=t_send.at[hop], recv_sem=t_recv.at[hop],
            device_id={"tp": (mt + hop) % tp}, device_id_type=MESH,
        )

    def squares():
        everything = nmall[...].astype(jnp.float32)
        parts = jnp.sum(jnp.sum(everything * everything, axis=0), axis=1)
        sums[0] = jnp.sum(parts, axis=1, keepdims=True) + jnp.zeros((2, LANES), jnp.float32)
        for hop in range(1, tp):
            t_copy(hop).start()

    def totals():
        result = sums[0]
        for hop in range(1, tp):
            t_copy(hop).wait_recv()
            result += sums[hop]
        tot_ref[...] = result

    def lows(start, count):
        for m in range(2):
            block = nmall[:, m].reshape(rank, cols).astype(jnp.bfloat16)
            product = jnp.dot(
                fall[start : start + count, m * rank : (m + 1) * rank], block, preferred_element_type=jnp.float32
            )
            for t in range(tiles_w):
                low[pl.ds(start * per_row + 2 * t + m, count, stride=per_row), :] = (
                    product[:, t * LANES : (t + 1) * LANES]
                )

    def weights(index, chunk, chunks):
        size = deep // chunks * per_row
        return wall.at[pl.ds(pl.multiple_of(index * deep * per_row + chunk * size, 16), size)]

    quarter = 2 * rank // tp
    if n == 8 and tp == 4 and quarter % LANES == 0 and deep % (2 * CHUNKS) == 0:
        place, parity = me // 2, me % 2
        flip = place // 2
        side = jnp.where(flip == 0, place, 3 - place)
        lists = Lists()
        states = [Weights(lists, q) for q in (0, 1)]
        partner = me + 1 - 2 * parity
        far, near = (mt + 2) % tp, mt + 1 - 2 * (mt % 2)

        def index_of(k, same):
            return 2 * (k + flip * (3 - 2 * k)) + (parity if same else 1 - parity)

        def target(q, way):
            return partner if way == "cross" else index_of(q + 1 if way == "up" else q - 1, True)

        ways = {"up": 0, "down": 1, "cross": 2}

        def w_copy(q, way, entry):
            k, same, chunk = entry
            index = index_of(k, same)
            return remote(
                weights(index, chunk, CHUNKS), w_send.at[ways[way]], w_recv.at[index, chunk],
                "fs", target(q, way),
            )

        def run(q, moves):
            for kind, way, entry in moves:
                if kind == "send":
                    w_copy(q, way, entry).start()
                else:
                    w_copy(q, "cross", entry).wait_recv()

        def piece(index, which):
            return fall.at[
                pl.ds(pl.multiple_of(index * deep, deep), deep), pl.ds(pl.multiple_of(which * quarter, quarter), quarter)
            ]

        def others(q):
            return sorted((k for k in range(4) if k != q), key=lambda k: (abs(k - q), k))

        def small(kind, index, to):
            if kind == "f":
                return remote(piece(index, mt), f_send.at[0], f_recv.at[index], "fs", to)
            return remote(nmall.at[index], n_send.at[0], n_recv.at[index], "fs", to)

        def small_begin(kind, q):
            for i, k in enumerate(reversed(others(q))):
                small(kind, me, index_of(k, True)).start()
            small(kind, me, partner).start()

        def spread(index, which, to, way):
            return remote(piece(index, which), s_send.at[0], s_recv.at[index, way], "tp", to)

        def small_wait(kind, q, k, same):
            index = index_of(k, same)
            small(kind, index, partner).wait_recv()
            if same:
                small(kind, index, partner).start()
            if kind == "f":
                spread(index, mt, far, 0).start()
                spread(index, mt, near, 1).start()

        def pieces(q):
            return [(q, False)] + [(k, True) for k in others(q)] + [(k, False) for k in others(q)]

        def place_of(k):
            return k + flip * (3 - 2 * k)

        def p_items(q):
            if q == 0:
                return [("down", 0, False), ("down", 0, True)]
            return [
                ("up", 3, False), ("up", 3, True), ("up", 2, False), ("down", 0, False), ("up", 2, True),
                ("down", 0, True), ("up", 1, False), ("down", 1, False), ("up", 1, True), ("down", 1, True),
            ]

        def p_slot(way, k, same):
            w = 0 if way == "up" else 1
            return (w + flip * (1 - 2 * w)) * 8 + place_of(k) * 2 + (0 if same else 1)

        def p_hop(q, way, k, same, src):
            slot = p_slot(way, k, same)
            to = min(max(q + (1 if way == "up" else -1), 0), 3)
            return pltpu.make_async_remote_copy(
                src_ref=src, dst_ref=pin.at[slot], send_sem=p_send.at[0], recv_sem=p_recv.at[slot],
                device_id={"fs": index_of(to, True)}, device_id_type=MESH,
            )

        def p_pass(q, way, k, same):
            slot = p_slot(way, k, same)
            p_hop(1, way, k, same, pin.at[slot]).wait_recv()
            if k != q:
                pmid[slot] = (
                    psend[index_of(k, same)].astype(jnp.float32) + pin[slot].astype(jnp.float32)
                ).astype(pmid.dtype)
                p_hop(q, way, k, same, pmid.at[slot]).start()

        def p_sum(q, same):
            total = psend[me if same else partner].astype(jnp.float32)
            for way, k, parity_same in p_items(q):
                if k == q and parity_same == same:
                    total += pin[p_slot(way, k, same)].astype(jnp.float32)
            return total

        def p_cross():
            return pltpu.make_async_remote_copy(
                src_ref=xsend, dst_ref=xrecv, send_sem=p_send.at[1], recv_sem=p_recv.at[16],
                device_id={"fs": partner}, device_id_type=MESH,
            )

        def gathered():
            p_cross().wait_recv()
            return ptot[...] + xrecv[...].astype(jnp.float32)

        def segment(tokens):
            for q in (0, 1):

                @pl.when(side == q)
                def _(q=q):
                    for token in tokens:
                        kind, *rest = token
                        if kind == "w":
                            run(q, states[q].take(*rest))
                        elif kind == "begin":
                            small_begin(rest[0], q)
                        elif kind == "pb" and q == 0:
                            for k in (3, 2, 1):
                                for same in (False, True):
                                    p_hop(q, "up", k, same, psend.at[index_of(k, same)]).start()
                        elif kind == "pd":
                            for i in rest[1 - q]:
                                p_pass(q, *p_items(q)[i])
                        elif kind == "pxs":
                            xsend[...] = p_sum(q, False).astype(xsend.dtype)
                            p_cross().start()
                        elif kind == "pt":
                            ptot[...] = p_sum(q, True)
                        elif kind == "small":
                            for i in rest[1]:
                                small_wait(rest[0], q, *pieces(q)[i])
                        elif kind == "all":
                            along, across, ahead = rest
                            while not states[q].done():
                                run(q, states[q].take(along, across, along + ahead, across + ahead))
                                along, across = along + 1, across + 1
                        elif kind == "spread":
                            for k, same in pieces(q):
                                index = index_of(k, same)
                                spread(index, far, far, 0).wait_recv()
                                spread(index, far, near, 2).start()
                            for k, same in pieces(q):
                                index = index_of(k, same)
                                spread(index, near, near, 1).wait_recv()
                                spread(index, (near + 2) % tp, near, 2).wait_recv()
                        elif kind == "sent":
                            for way in ways:
                                if states[q].out[way]:
                                    all_sent(wall, w_send.at[ways[way]], len(states[q].out[way]), CHUNKS)

        def all_sent(whole, sem, count, per_block):
            rows = whole.shape[0] // n // per_block * count
            part = whole.at[pl.ds(0, rows)]
            remote(part, sem, sem, "fs", partner).wait_send()

        def rest_sent():
            all_sent(fall, f_send.at[0], 7, tp)
            all_sent(fall, s_send.at[0], 21, tp)
            all_sent(nmall, n_send.at[0], 7, 1)
            remote(pmid.at[pl.ds(0, 6)], p_send.at[0], p_send.at[0], "fs", partner).wait_send()
            p_cross().wait_send()

        computes = {
            "own": own_weights, "project": project, "squares": squares, "totals": totals, "momentum": lambda: momentum(gathered()),
            "lows": lambda j: lows(j * deep, deep),
        }
        pl.semaphore_wait(barrier, n - 1 + tp - 1)
        for token in SCHEDULE:
            if token[0] == "head":
                for i in range(token[1], heads if token[1] == 3 else token[1] + 1):
                    head(i)
            elif token[0] in computes:
                computes[token[0]](*token[1:])
            else:
                segment([token])
        segment([("sent",)])
        rest_sent()
    else:
        own_weights()
        for i in range(heads):
            head(i)
        pl.semaphore_wait(barrier, n - 1 + tp - 1)

        def block(kind, index, hop):
            if kind == "f":
                return remote(
                    fall.at[pl.ds(pl.multiple_of(index * deep, 8), deep)], f_send.at[hop], f_recv.at[index],
                    "fs", (me + hop) % n,
                )
            if kind == "w":
                return remote(weights(index, 0, 1), w_send.at[hop], w_recv.at[index], "fs", (me + hop) % n)
            return remote(nmall.at[index], n_send.at[hop], n_recv.at[index], "fs", (me + hop) % n)

        def each(action):
            def step(hop, carry):
                action(hop)
                return carry

            lax.fori_loop(1, n, step, 0)

        each(lambda hop: block("f", me, hop).start())
        each(lambda hop: block("w", me, hop).start())
        each(lambda hop: block("f", (me + hop) % n, hop).wait_recv())
        project()
        each(lambda hop: p_copy(hop).start())

        def add(hop, total):
            p_copy(hop).wait_recv()
            return total + precv[hop].astype(jnp.float32)

        momentum(lax.fori_loop(1, n, add, psend[me].astype(jnp.float32)))
        each(lambda hop: block("n", me, hop).start())
        each(lambda hop: block("n", (me + hop) % n, hop).wait_recv())
        squares()
        for start in range(0, depth, 256):
            lows(start, min(256, depth - start))
        totals()
        each(lambda hop: block("w", (me + hop) % n, hop).wait_recv())
        for kind in ("f", "w", "n"):
            each(lambda hop, kind=kind: block(kind, me, hop).wait_send())
        each(lambda hop: p_copy(hop).wait_send())
    for hop in range(1, tp):
        t_copy(hop).wait_send()


def finish(n, entries, wall, low, nm_ref, tot_ref, step_hbm, nm_hbm, copies_hbm, step, copies, sems):
    me = lax.axis_index("fs")
    rows = low.shape[0]
    own = rows // n
    nm_copy = pltpu.make_async_copy(nm_ref, nm_hbm, sems.at[0])
    nm_copy.start()
    rate = RATE_BASE / jnp.sqrt(1.0 + tot_ref[...] / entries)
    count = min(rows // 16, 1024)
    odd = lax.broadcasted_iota(jnp.int32, (8, LANES), 0) % 2 == 1
    rates = jnp.where(odd, rate[1:2], rate[0:1])[None]
    started = [nm_copy]

    def scaled(start, size):
        return (low[pl.ds(start, size), :].reshape(size // 8, 8, LANES) * rates).reshape(size, LANES)

    for i in range(rows // count):
        at = slice(i * count, (i + 1) * count)
        copies[at, :] = (wall[at, :].astype(jnp.float32) - scaled(i * count, count)).astype(jnp.bfloat16)
        started.append(pltpu.make_async_copy(copies.at[at], copies_hbm.at[at], sems.at[2 + i]))
        started[-1].start()
        if i == 1:
            for first in range(0, own, min(count, own)):
                size = min(count, own)
                step[first : first + size, :] = scaled(pl.multiple_of(me * own + first, 8), size)
            started.append(pltpu.make_async_copy(step, step_hbm, sems.at[1]))
            started[-1].start()
    for copy in started:
        copy.wait()


def to_rows(array):
    rows, maps, cols = array.shape
    return array.reshape(rows, maps, cols // LANES, LANES).transpose(0, 2, 1, 3).reshape(-1, LANES)


def from_rows(array, rows):
    return (
        array.reshape(rows, -1, 2, LANES).transpose(0, 2, 1, 3).reshape(rows, 2, -1)
    )


def per_device(
    n, tp, inputs, queries, keys, values, head_cot, mixing, head_gain, factors, moments, weights
):
    length, depth = inputs.shape
    heads = mixing.shape[0]
    deep, _, rank = factors.shape
    rank_here, _, cols = moments.shape
    wire = jnp.bfloat16 if rank_here % 16 == 0 else jnp.float32
    per_row = 2 * cols // LANES
    hbm = pl.BlockSpec(memory_space=pltpu.HBM)
    vmem = pl.BlockSpec(memory_space=pltpu.VMEM)
    dma = pltpu.SemaphoreType.DMA
    args = (
        inputs, queries, keys, values, head_cot, mixing, head_gain[None, :],
        to_rows(factors), to_rows(moments), to_rows(weights),
    )
    semaphores = [
            dma((len(args),)),
            *(
                (
                    dma((1,)), dma((n,)), dma((1,)), dma((n, 3)),
                    dma((3,)), dma((n, CHUNKS)), dma((1,)), dma((n,)), dma((2,)), dma((17,)),
                )
                if n == 8
                else (dma((n,)), dma((n,)), dma((1,)), dma((1,)), dma((n,)), dma((n,)), dma((n,)), dma((n,)), dma((n,)), dma((n,)))
            ),
            dma((tp,)), dma((tp,)),
    ]

    def scoped(*refs):
        pl.run_scoped(lambda *sems: kernel(n, tp, heads, *refs, *sems), *semaphores)

    held = pl.pallas_call(
        scoped,
        out_shape=(
            pltpu.VMEM((depth * per_row, LANES), jnp.bfloat16),
            pltpu.VMEM((depth * per_row, LANES), jnp.float32),
            pltpu.VMEM((rank_here * per_row, LANES), jnp.float32),
            pltpu.VMEM((2, LANES), jnp.float32),
        ),
        in_specs=[hbm] * len(args),
        out_specs=(vmem,) * 4,
        scratch_shapes=[
            pltpu.VMEM((length, depth), jnp.bfloat16),
            pltpu.VMEM((length, cols), jnp.bfloat16),
            pltpu.VMEM((length, cols), jnp.bfloat16),
            pltpu.VMEM((length, cols), jnp.bfloat16),
            pltpu.VMEM((length, cols), jnp.bfloat16),
            pltpu.SMEM((heads,), jnp.float32),
            pltpu.VMEM((1, head_gain.shape[0]), jnp.float32),
            pltpu.VMEM((deep * 2 * rank // LANES, LANES), jnp.bfloat16),
            pltpu.VMEM((rank_here * per_row, LANES), jnp.float32),
            pltpu.VMEM((deep * per_row, LANES), jnp.float32),
            pltpu.VMEM((depth, 2 * rank), jnp.bfloat16),
            pltpu.VMEM((n, 2, rank_here, cols), wire),
            pltpu.VMEM((deep * 2 * rank // LANES, LANES), jnp.float32),
            pltpu.VMEM((length, cols), jnp.bfloat16),
            pltpu.VMEM((length, cols), jnp.bfloat16),
            pltpu.VMEM((n, 2, rank_here, cols), wire),
            pltpu.VMEM((n, 2, rank_here, cols), wire),
            pltpu.VMEM((16 if n == 8 else 1, 2, rank_here, cols), wire),
            pltpu.VMEM((16 if n == 8 else 1, 2, rank_here, cols), wire),
            pltpu.VMEM((2, rank_here, cols), wire),
            pltpu.VMEM((2, rank_here, cols), wire),
            pltpu.VMEM((2, rank_here, cols), jnp.float32),
            pltpu.VMEM((tp, 2, LANES), jnp.float32),
        ],
        compiler_params=pltpu.CompilerParams(
            collective_id=0, has_side_effects=True, vmem_limit_bytes=36 * 1024 * 1024
        ),
    )(*(pltpu.with_memory_space_constraint(arg, pltpu.HBM) for arg in args))
    out_hbm = pl.BlockSpec(memory_space=pltpu.HBM)
    step, new_moments, copies = pl.pallas_call(
        functools.partial(finish, n, rank * cols * tp),
        out_shape=(
            jax.ShapeDtypeStruct((deep * per_row, LANES), jnp.float32),
            jax.ShapeDtypeStruct((rank_here * per_row, LANES), jnp.float32),
            jax.ShapeDtypeStruct((depth * per_row, LANES), jnp.bfloat16),
        ),
        in_specs=[vmem] * 4,
        out_specs=(out_hbm,) * 3,
        scratch_shapes=[
            pltpu.VMEM((deep * per_row, LANES), jnp.float32),
            pltpu.VMEM((depth * per_row, LANES), jnp.bfloat16),
            dma((18,)),
        ],
        compiler_params=pltpu.CompilerParams(vmem_limit_bytes=16 * 1024 * 1024),
    )(*held)
    return from_rows(step, deep), from_rows(new_moments, rank_here), from_rows(copies, depth)


def solution(mesh):
    placed = (
        P("fs", None),
        P("fs", "tp"),
        P("fs", "tp"),
        P("fs", "tp"),
        P("fs", "tp"),
        P("tp"),
        P(),
        P("fs", None, None),
        P("fs", None, "tp"),
        P("fs", None, "tp"),
    )
    return jax.shard_map(
        functools.partial(per_device, mesh.shape["fs"], mesh.shape["tp"]),
        mesh=mesh,
        in_specs=placed,
        out_specs=(P("fs", None, "tp"), P("fs", None, "tp"), P(None, None, "tp")),
        check_vma=False,
    )
```

```python
import functools

import jax
import jax.numpy as jnp
from jax import lax
from jax.experimental import pallas as pl
from jax.experimental.pallas import tpu as pltpu
from jax.sharding import PartitionSpec as P

EPS = 0.05
BETA = 0.9
RATE_BASE = 0.5
MESH = pl.DeviceIdType.MESH
LANES = 128
CHUNKS = 16
WIDE = 3
SCHEDULE = [
    ("begin", "f"), ("own",), ("w", 0, 0, 93, 9), ("small", "f", (0,)), ("small", "f", (3,)), ("small", "f", (1,)),
    ("small", "f", (2,)), ("head", 0), ("w", 1, 0, 92, 4), ("w", 0, 0, 92, 4), ("w", 0, 0, 75, 10),
    ("w", 0, 2, 77, 14), ("w", 1, 2, 74, 16), ("head", 1), ("w", 2, 2, 77, 17), ("small", "f", (6,)), ("head", 2),
    ("w", 0, 9, 45, 67), ("small", "f", (4,)), ("head", 3), ("small", "f", (5,)), ("w", 7, 10, 42, 60),
    ("w", 9, 0, 52, 0), ("spread",), ("project",), ("w", 7, 5, 42, 57), ("pb",), ("pd", (0,), ()), ("pd", (1,), ()),
    ("w", 2, 2, 53, 59), ("w", 16, 6, 31, 53), ("w", 28, 7, 29, 44), ("pd", (2,), ()), ("pd", (3,), (0,)),
    ("w", 0, 11, 25, 24), ("pd", (4,), ()), ("pd", (5,), (1,)), ("w", 22, 33, 43, 46), ("pd", (6,), ()),
    ("pd", (7,), ()), ("pxs",), ("pd", (8,), ()), ("pd", (9,), ()), ("pt",), ("w", 24, 30, 35, 59),
    ("w", 22, 17, 63, 39), ("w", 23, 38, 64, 47), ("w", 16, 32, 55, 43), ("w", 19, 27, 65, 49), ("momentum",),
    ("begin", "n"), ("w", 46, 26, 33, 95), ("small", "n", (0,)), ("small", "n", (3,)), ("w", 19, 46, 71, 37),
    ("small", "n", (2,)), ("small", "n", (1,)), ("w", 51, 32, 20, 53), ("w", 52, 23, 24, 67), ("small", "n", (5,)),
    ("small", "n", (4,)), ("small", "n", (6,)), ("squares",), ("w", 41, 35, 22, 57), ("lows", 0), ("lows", 1),
    ("lows", 2), ("w", 39, 31, 41, 52), ("lows", 3), ("w", 53, 30, 24, 52), ("w", 54, 23, 21, 48), ("lows", 4),
    ("lows", 5), ("w", 55, 23, 21, 48), ("lows", 6), ("lows", 7), ("totals",), ("all", 117, 122, 81),
]


def split(ref, t, tiles, count):
    return ref[pl.ds(t % tiles * 2 + t // tiles, count, stride=2 * tiles), :]


def head_step(head, q_ref, k_ref, v_ref, c_ref, mix_ref, gain_ref, dq_ref, dv_ref):
    length = q_ref.shape[0]
    width = gain_ref.shape[1]
    half = width // 2
    factor = half ** (-0.5)
    cols = slice(head * width, (head + 1) * width)
    query, key, value = q_ref[:, cols], k_ref[:, cols], v_ref[:, cols]
    lane = lax.broadcasted_iota(jnp.int32, (length, width), 1)
    zero = jnp.zeros_like(key)
    key0 = jnp.where(lane < half, key, zero)
    key1 = jnp.where(lane < half, zero, key)
    row = lax.broadcasted_iota(jnp.int32, (length, length), 0)
    col = lax.broadcasted_iota(jnp.int32, (length, length), 1)
    causal = col <= row
    mix = mix_ref[head]
    nt = (((1,), (1,)), ((), ()))
    tn = (((0,), (0,)), ((), ()))

    def probs(rows):
        scores = lax.dot_general(query, rows, nt, preferred_element_type=jnp.float32) * factor
        scores = jnp.where(causal, scores, -jnp.inf)
        expo = jnp.exp(scores - jnp.max(scores, axis=-1, keepdims=True))
        return expo * (1.0 / jnp.sum(expo, axis=-1, keepdims=True))

    first, second = probs(key0), probs(key1)
    mixed = (first - mix * second).astype(jnp.bfloat16)
    output = jnp.dot(mixed, value, preferred_element_type=jnp.float32)
    inverse = lax.rsqrt(jnp.mean(output * output, axis=-1, keepdims=True) + EPS)
    scaled = gain_ref[...] * c_ref[:, cols].astype(jnp.float32)
    d_out = inverse * scaled - output * (inverse * inverse * inverse) * jnp.mean(
        output * scaled, axis=-1, keepdims=True
    )
    d_out = d_out.astype(jnp.bfloat16)
    dv_ref[:, cols] = lax.dot_general(mixed, d_out, tn, preferred_element_type=jnp.float32).astype(jnp.bfloat16)
    d_mix = lax.dot_general(d_out, value, nt, preferred_element_type=jnp.float32)
    d_first = first * (d_mix - jnp.sum(first * d_mix, axis=-1, keepdims=True))
    d_second = -mix * second * (d_mix - jnp.sum(second * d_mix, axis=-1, keepdims=True))
    d_query = jnp.dot(d_first.astype(jnp.bfloat16), key0, preferred_element_type=jnp.float32)
    d_query += jnp.dot(d_second.astype(jnp.bfloat16), key1, preferred_element_type=jnp.float32)
    dq_ref[:, cols] = (d_query * factor).astype(jnp.bfloat16)


class Lists:
    def __init__(self):
        def source(k, order):
            return [(k, True, c) for c in order] + [(k, False, c) for c in range(WIDE)]

        order = list(range(WIDE, CHUNKS)) + list(range(WIDE))
        mirror = lambda entries: [(3 - k, same, c) for k, same, c in entries]
        first = source(0, order)
        inner = source(1, order)
        self.up = {0: first, 1: self.merge(inner, first)}
        far = mirror(self.up[1])
        self.down = {0: [], 1: self.merge(inner, far)}
        self.from_up = {0: self.down[1], 1: far}
        self.from_down = {0: [], 1: first}
        own = lambda q: [(q, True, c) for c in range(CHUNKS)]
        narrow = lambda entries: [e for e in entries if e[1] and e[2] >= WIDE]
        self.cross = {
            0: own(0) + narrow(self.from_up[0]),
            1: own(1) + self.weave(narrow(self.from_down[1]), narrow(self.from_up[1])),
        }
        self.from_cross = {q: [(k, not same, c) for k, same, c in self.cross[q]] for q in (0, 1)}

    @staticmethod
    def merge(own, passed):
        return own + passed

    @staticmethod
    def weave(a, b):
        out = []
        for i in range(max(len(a), len(b))):
            out += a[i : i + 1] + b[i : i + 1]
        return out


class Weights:
    def __init__(self, lists, q):
        self.q = q
        self.out = {"up": list(lists.up[q]), "down": list(lists.down[q]), "cross": list(lists.cross[q])}
        self.into = {
            "cross": list(lists.from_cross[q]), "down": list(lists.from_down[q]), "up": list(lists.from_up[q]),
        }
        self.have = {(q, True, c) for c in range(CHUNKS)}
        self.got = {way: 0 for way in self.into}
        self.put = {way: 0 for way in self.out}

    def push(self, along, across):
        moves = []
        for way, goal in (("up", along), ("down", along), ("cross", across)):
            while self.put[way] < min(len(self.out[way]), goal):
                entry = self.out[way][self.put[way]]
                if entry not in self.have:
                    break
                moves.append(("send", way, entry))
                self.put[way] += 1
        return moves

    def take(self, along, across, push_along, push_across):
        moves = self.push(push_along, push_across)
        goals = {"cross": across, "down": along, "up": along}
        for count in range(1, max(along, across) + 1):
            for way, goal in goals.items():
                if self.got[way] < min(len(self.into[way]), goal, count):
                    entry = self.into[way][self.got[way]]
                    moves.append(("wait", way, entry))
                    self.have.add(entry)
                    self.got[way] += 1
                    moves += self.push(push_along, push_across)
        return moves

    def done(self):
        return all(self.got[w] == len(self.into[w]) for w in self.into) and all(
            self.put[w] == len(self.out[w]) for w in self.out
        )


def kernel(
    n, tp, heads,
    x_hbm, q_hbm, k_hbm, v_hbm, c_hbm, mix_hbm, gain_hbm, f_hbm, mom_hbm, w_hbm,
    wall, low, nm_ref, tot_ref,
    x_ref, q_ref, k_ref, v_ref, c_ref, mix_ref, gain_ref, f_ref, mom_ref, w_ref,
    fall, nmall, fwide, dq, dv, psend, precv, pin, pmid, xsend, xrecv, ptot, sums,
    l_sem, f_send, f_recv, s_send, s_recv, w_send, w_recv, n_send, n_recv, p_send, p_recv, t_send, t_recv,
):
    me = lax.axis_index("fs")
    mt = lax.axis_index("tp")
    depth = fall.shape[0]
    deep = depth // n
    rank = fall.shape[1] // 2
    rank_here = rank // n
    cols = dq.shape[1]
    tiles_f, tiles_w = rank // LANES, cols // LANES
    per_row = 2 * tiles_w

    local = {}
    for i, (name, src, dst) in enumerate((
        ("f", f_hbm, f_ref), ("w", w_hbm, w_ref), ("gain", gain_hbm, gain_ref), ("mix", mix_hbm, mix_ref),
        ("q", q_hbm, q_ref), ("k", k_hbm, k_ref), ("v", v_hbm, v_ref), ("c", c_hbm, c_ref),
        ("x", x_hbm, x_ref), ("mom", mom_hbm, mom_ref),
    )):
        local[name] = pltpu.make_async_copy(src, dst, l_sem.at[i])
        local[name].start()

    barrier = pltpu.get_barrier_semaphore()
    for hop in range(1, n):
        pl.semaphore_signal(barrier, inc=1, device_id={"fs": (me + hop) % n}, device_id_type=MESH)
    for hop in range(1, tp):
        pl.semaphore_signal(barrier, inc=1, device_id={"tp": (mt + hop) % tp}, device_id_type=MESH)

    local["f"].wait()
    fwide[...] = f_ref[...].astype(jnp.float32)
    here = pl.ds(pl.multiple_of(me * deep, deep), deep)
    for t in range(2 * tiles_f):
        fall[here, t * LANES : (t + 1) * LANES] = split(fwide, t, tiles_f, deep).astype(jnp.bfloat16)

    def own_weights():
        local["w"].wait()
        wall[pl.ds(pl.multiple_of(me * deep * per_row, 16), deep * per_row), :] = w_ref[...].astype(jnp.bfloat16)

    def head(i):
        if i == 0:
            for name in ("gain", "mix", "q", "k", "v", "c"):
                local[name].wait()
        head_step(i, q_ref, k_ref, v_ref, c_ref, mix_ref, gain_ref, dq, dv)

    def remote(src, send, recv, axis, target):
        return pltpu.make_async_remote_copy(
            src_ref=src, dst_ref=src, send_sem=send, recv_sem=recv, device_id={axis: target}, device_id_type=MESH
        )

    def project():
        local["x"].wait()
        for m, cot in enumerate((dq, dv)):
            reduced = jnp.dot(
                x_ref[...], fall[:, m * rank : (m + 1) * rank], preferred_element_type=jnp.float32
            ).astype(jnp.bfloat16)
            partial = lax.dot_general(
                reduced, cot[...], (((0,), (0,)), ((), ())), preferred_element_type=jnp.float32
            )
            for j in range(n):
                psend[j, m] = partial[j * rank_here : (j + 1) * rank_here].astype(psend.dtype)

    def p_copy(hop):
        peer = (me + hop) % n
        return pltpu.make_async_remote_copy(
            src_ref=psend.at[peer], dst_ref=precv.at[hop], send_sem=p_send.at[hop], recv_sem=p_recv.at[hop],
            device_id={"fs": peer}, device_id_type=MESH,
        )

    def momentum(total):
        local["mom"].wait()
        length = x_ref.shape[0]
        for t in range(2 * tiles_w):
            m, lanes = t // tiles_w, slice(t % tiles_w * LANES, (t % tiles_w + 1) * LANES)
            moments = BETA * split(mom_ref, t, tiles_w, rank_here)
            moments += total[m, :, lanes] * (length * n) ** (-0.5)
            nm_ref[pl.ds(t % tiles_w * 2 + m, rank_here, stride=per_row), :] = moments
            nmall[me, m, :, lanes] = moments.astype(nmall.dtype)

    def t_copy(hop):
        return pltpu.make_async_remote_copy(
            src_ref=sums.at[0], dst_ref=sums.at[hop], send_sem=t_send.at[hop], recv_sem=t_recv.at[hop],
            device_id={"tp": (mt + hop) % tp}, device_id_type=MESH,
        )

    def squares():
        everything = nmall[...].astype(jnp.float32)
        parts = jnp.sum(jnp.sum(everything * everything, axis=0), axis=1)
        sums[0] = jnp.sum(parts, axis=1, keepdims=True) + jnp.zeros((2, LANES), jnp.float32)
        for hop in range(1, tp):
            t_copy(hop).start()

    def totals():
        result = sums[0]
        for hop in range(1, tp):
            t_copy(hop).wait_recv()
            result += sums[hop]
        tot_ref[...] = result

    def lows(start, count):
        for m in range(2):
            block = nmall[:, m].reshape(rank, cols).astype(jnp.bfloat16)
            product = jnp.dot(
                fall[start : start + count, m * rank : (m + 1) * rank], block, preferred_element_type=jnp.float32
            )
            for t in range(tiles_w):
                low[pl.ds(start * per_row + 2 * t + m, count, stride=per_row), :] = (
                    product[:, t * LANES : (t + 1) * LANES]
                )

    def weights(index, chunk, chunks):
        size = deep // chunks * per_row
        return wall.at[pl.ds(pl.multiple_of(index * deep * per_row + chunk * size, 16), size)]

    quarter = 2 * rank // tp
    if n == 8 and tp == 4 and quarter % LANES == 0 and deep % (2 * CHUNKS) == 0:
        place, parity = me // 2, me % 2
        flip = place // 2
        side = jnp.where(flip == 0, place, 3 - place)
        lists = Lists()
        states = [Weights(lists, q) for q in (0, 1)]
        partner = me + 1 - 2 * parity
        far, near = (mt + 2) % tp, mt + 1 - 2 * (mt % 2)

        def index_of(k, same):
            return 2 * (k + flip * (3 - 2 * k)) + (parity if same else 1 - parity)

        def target(q, way):
            return partner if way == "cross" else index_of(q + 1 if way == "up" else q - 1, True)

        ways = {"up": 0, "down": 1, "cross": 2}

        def w_copy(q, way, entry):
            k, same, chunk = entry
            index = index_of(k, same)
            return remote(
                weights(index, chunk, CHUNKS), w_send.at[ways[way]], w_recv.at[index, chunk],
                "fs", target(q, way),
            )

        def run(q, moves):
            for kind, way, entry in moves:
                if kind == "send":
                    w_copy(q, way, entry).start()
                else:
                    w_copy(q, "cross", entry).wait_recv()

        def piece(index, which):
            return fall.at[
                pl.ds(pl.multiple_of(index * deep, deep), deep), pl.ds(pl.multiple_of(which * quarter, quarter), quarter)
            ]

        def others(q):
            return sorted((k for k in range(4) if k != q), key=lambda k: (abs(k - q), k))

        def small(kind, index, to):
            if kind == "f":
                return remote(piece(index, mt), f_send.at[0], f_recv.at[index], "fs", to)
            return remote(nmall.at[index], n_send.at[0], n_recv.at[index], "fs", to)

        def small_begin(kind, q):
            for i, k in enumerate(reversed(others(q))):
                small(kind, me, index_of(k, True)).start()
            small(kind, me, partner).start()

        def spread(index, which, to, way):
            return remote(piece(index, which), s_send.at[0], s_recv.at[index, way], "tp", to)

        def small_wait(kind, q, k, same):
            index = index_of(k, same)
            small(kind, index, partner).wait_recv()
            if same:
                small(kind, index, partner).start()
            if kind == "f":
                spread(index, mt, far, 0).start()
                spread(index, mt, near, 1).start()

        def pieces(q):
            return [(q, False)] + [(k, True) for k in others(q)] + [(k, False) for k in others(q)]

        def place_of(k):
            return k + flip * (3 - 2 * k)

        def p_items(q):
            if q == 0:
                return [("down", 0, False), ("down", 0, True)]
            return [
                ("up", 3, False), ("up", 3, True), ("up", 2, False), ("down", 0, False), ("up", 2, True),
                ("down", 0, True), ("up", 1, False), ("down", 1, False), ("up", 1, True), ("down", 1, True),
            ]

        def p_slot(way, k, same):
            w = 0 if way == "up" else 1
            return (w + flip * (1 - 2 * w)) * 8 + place_of(k) * 2 + (0 if same else 1)

        def p_hop(q, way, k, same, src):
            slot = p_slot(way, k, same)
            to = min(max(q + (1 if way == "up" else -1), 0), 3)
            return pltpu.make_async_remote_copy(
                src_ref=src, dst_ref=pin.at[slot], send_sem=p_send.at[0], recv_sem=p_recv.at[slot],
                device_id={"fs": index_of(to, True)}, device_id_type=MESH,
            )

        def p_pass(q, way, k, same):
            slot = p_slot(way, k, same)
            p_hop(1, way, k, same, pin.at[slot]).wait_recv()
            if k != q:
                pmid[slot] = (
                    psend[index_of(k, same)].astype(jnp.float32) + pin[slot].astype(jnp.float32)
                ).astype(pmid.dtype)
                p_hop(q, way, k, same, pmid.at[slot]).start()

        def p_sum(q, same):
            total = psend[me if same else partner].astype(jnp.float32)
            for way, k, parity_same in p_items(q):
                if k == q and parity_same == same:
                    total += pin[p_slot(way, k, same)].astype(jnp.float32)
            return total

        def p_cross():
            return pltpu.make_async_remote_copy(
                src_ref=xsend, dst_ref=xrecv, send_sem=p_send.at[1], recv_sem=p_recv.at[16],
                device_id={"fs": partner}, device_id_type=MESH,
            )

        def gathered():
            p_cross().wait_recv()
            return ptot[...] + xrecv[...].astype(jnp.float32)

        def segment(tokens):
            for q in (0, 1):

                @pl.when(side == q)
                def _(q=q):
                    for token in tokens:
                        kind, *rest = token
                        if kind == "w":
                            run(q, states[q].take(*rest))
                        elif kind == "begin":
                            small_begin(rest[0], q)
                        elif kind == "pb" and q == 0:
                            for k in (3, 2, 1):
                                for same in (False, True):
                                    p_hop(q, "up", k, same, psend.at[index_of(k, same)]).start()
                        elif kind == "pd":
                            for i in rest[1 - q]:
                                p_pass(q, *p_items(q)[i])
                        elif kind == "pxs":
                            xsend[...] = p_sum(q, False).astype(xsend.dtype)
                            p_cross().start()
                        elif kind == "pt":
                            ptot[...] = p_sum(q, True)
                        elif kind == "small":
                            for i in rest[1]:
                                small_wait(rest[0], q, *pieces(q)[i])
                        elif kind == "all":
                            along, across, ahead = rest
                            while not states[q].done():
                                run(q, states[q].take(along, across, along + ahead, across + ahead))
                                along, across = along + 1, across + 1
                        elif kind == "spread":
                            for k, same in pieces(q):
                                index = index_of(k, same)
                                spread(index, far, far, 0).wait_recv()
                                spread(index, far, near, 2).start()
                            for k, same in pieces(q):
                                index = index_of(k, same)
                                spread(index, near, near, 1).wait_recv()
                                spread(index, (near + 2) % tp, near, 2).wait_recv()
                        elif kind == "sent":
                            for way in ways:
                                if states[q].out[way]:
                                    all_sent(wall, w_send.at[ways[way]], len(states[q].out[way]), CHUNKS)

        def all_sent(whole, sem, count, per_block):
            rows = whole.shape[0] // n // per_block * count
            part = whole.at[pl.ds(0, rows)]
            remote(part, sem, sem, "fs", partner).wait_send()

        def rest_sent():
            all_sent(fall, f_send.at[0], 7, tp)
            all_sent(fall, s_send.at[0], 21, tp)
            all_sent(nmall, n_send.at[0], 7, 1)
            remote(pmid.at[pl.ds(0, 6)], p_send.at[0], p_send.at[0], "fs", partner).wait_send()
            p_cross().wait_send()

        computes = {
            "own": own_weights, "project": project, "squares": squares, "totals": totals, "momentum": lambda: momentum(gathered()),
            "lows": lambda j: lows(j * deep, 4 * deep) if j % 4 == 0 else None,
        }
        pl.semaphore_wait(barrier, n - 1 + tp - 1)
        for token in SCHEDULE:
            if token[0] == "head":
                for i in range(token[1], heads if token[1] == 3 else token[1] + 1):
                    head(i)
            elif token[0] in computes:
                computes[token[0]](*token[1:])
            else:
                segment([token])
        segment([("sent",)])
        rest_sent()
    else:
        own_weights()
        for i in range(heads):
            head(i)
        pl.semaphore_wait(barrier, n - 1 + tp - 1)

        def block(kind, index, hop):
            if kind == "f":
                return remote(
                    fall.at[pl.ds(pl.multiple_of(index * deep, 8), deep)], f_send.at[hop], f_recv.at[index],
                    "fs", (me + hop) % n,
                )
            if kind == "w":
                return remote(weights(index, 0, 1), w_send.at[hop], w_recv.at[index], "fs", (me + hop) % n)
            return remote(nmall.at[index], n_send.at[hop], n_recv.at[index], "fs", (me + hop) % n)

        def each(action):
            def step(hop, carry):
                action(hop)
                return carry

            lax.fori_loop(1, n, step, 0)

        each(lambda hop: block("f", me, hop).start())
        each(lambda hop: block("w", me, hop).start())
        each(lambda hop: block("f", (me + hop) % n, hop).wait_recv())
        project()
        each(lambda hop: p_copy(hop).start())

        def add(hop, total):
            p_copy(hop).wait_recv()
            return total + precv[hop].astype(jnp.float32)

        momentum(lax.fori_loop(1, n, add, psend[me].astype(jnp.float32)))
        each(lambda hop: block("n", me, hop).start())
        each(lambda hop: block("n", (me + hop) % n, hop).wait_recv())
        squares()
        for start in range(0, depth, 256):
            lows(start, min(256, depth - start))
        totals()
        each(lambda hop: block("w", (me + hop) % n, hop).wait_recv())
        for kind in ("f", "w", "n"):
            each(lambda hop, kind=kind: block(kind, me, hop).wait_send())
        each(lambda hop: p_copy(hop).wait_send())
    for hop in range(1, tp):
        t_copy(hop).wait_send()


def finish(n, entries, wall, low, nm_ref, tot_ref, step_hbm, nm_hbm, copies_hbm, step, copies, sems):
    me = lax.axis_index("fs")
    rows = low.shape[0]
    own = rows // n
    nm_copy = pltpu.make_async_copy(nm_ref, nm_hbm, sems.at[0])
    nm_copy.start()
    rate = RATE_BASE / jnp.sqrt(1.0 + tot_ref[...] / entries)
    count = min(rows // 16, 1024)
    odd = lax.broadcasted_iota(jnp.int32, (8, LANES), 0) % 2 == 1
    rates = jnp.where(odd, rate[1:2], rate[0:1])[None]
    started = [nm_copy]

    def scaled(start, size):
        return (low[pl.ds(start, size), :].reshape(size // 8, 8, LANES) * rates).reshape(size, LANES)

    for i in range(rows // count):
        at = slice(i * count, (i + 1) * count)
        copies[at, :] = (wall[at, :].astype(jnp.float32) - scaled(i * count, count)).astype(jnp.bfloat16)
        started.append(pltpu.make_async_copy(copies.at[at], copies_hbm.at[at], sems.at[2 + i]))
        started[-1].start()
        if i == 1:
            for first in range(0, own, min(count, own)):
                size = min(count, own)
                step[first : first + size, :] = scaled(pl.multiple_of(me * own + first, 8), size)
            started.append(pltpu.make_async_copy(step, step_hbm, sems.at[1]))
            started[-1].start()
    for copy in started:
        copy.wait()


def to_rows(array):
    rows, maps, cols = array.shape
    return array.reshape(rows, maps, cols // LANES, LANES).transpose(0, 2, 1, 3).reshape(-1, LANES)


def from_rows(array, rows):
    return (
        array.reshape(rows, -1, 2, LANES).transpose(0, 2, 1, 3).reshape(rows, 2, -1)
    )


def per_device(
    n, tp, inputs, queries, keys, values, head_cot, mixing, head_gain, factors, moments, weights
):
    length, depth = inputs.shape
    heads = mixing.shape[0]
    deep, _, rank = factors.shape
    rank_here, _, cols = moments.shape
    wire = jnp.bfloat16 if rank_here % 16 == 0 else jnp.float32
    per_row = 2 * cols // LANES
    hbm = pl.BlockSpec(memory_space=pltpu.HBM)
    vmem = pl.BlockSpec(memory_space=pltpu.VMEM)
    dma = pltpu.SemaphoreType.DMA
    args = (
        inputs, queries, keys, values, head_cot, mixing, head_gain[None, :],
        to_rows(factors), to_rows(moments), to_rows(weights),
    )
    semaphores = [
            dma((len(args),)),
            *(
                (
                    dma((1,)), dma((n,)), dma((1,)), dma((n, 3)),
                    dma((3,)), dma((n, CHUNKS)), dma((1,)), dma((n,)), dma((2,)), dma((17,)),
                )
                if n == 8
                else (dma((n,)), dma((n,)), dma((1,)), dma((1,)), dma((n,)), dma((n,)), dma((n,)), dma((n,)), dma((n,)), dma((n,)))
            ),
            dma((tp,)), dma((tp,)),
    ]

    def scoped(*refs):
        pl.run_scoped(lambda *sems: kernel(n, tp, heads, *refs, *sems), *semaphores)

    held = pl.pallas_call(
        scoped,
        out_shape=(
            pltpu.VMEM((depth * per_row, LANES), jnp.bfloat16),
            pltpu.VMEM((depth * per_row, LANES), jnp.float32),
            pltpu.VMEM((rank_here * per_row, LANES), jnp.float32),
            pltpu.VMEM((2, LANES), jnp.float32),
        ),
        in_specs=[hbm] * len(args),
        out_specs=(vmem,) * 4,
        scratch_shapes=[
            pltpu.VMEM((length, depth), jnp.bfloat16),
            pltpu.VMEM((length, cols), jnp.bfloat16),
            pltpu.VMEM((length, cols), jnp.bfloat16),
            pltpu.VMEM((length, cols), jnp.bfloat16),
            pltpu.VMEM((length, cols), jnp.bfloat16),
            pltpu.SMEM((heads,), jnp.float32),
            pltpu.VMEM((1, head_gain.shape[0]), jnp.float32),
            pltpu.VMEM((deep * 2 * rank // LANES, LANES), jnp.bfloat16),
            pltpu.VMEM((rank_here * per_row, LANES), jnp.float32),
            pltpu.VMEM((deep * per_row, LANES), jnp.float32),
            pltpu.VMEM((depth, 2 * rank), jnp.bfloat16),
            pltpu.VMEM((n, 2, rank_here, cols), wire),
            pltpu.VMEM((deep * 2 * rank // LANES, LANES), jnp.float32),
            pltpu.VMEM((length, cols), jnp.bfloat16),
            pltpu.VMEM((length, cols), jnp.bfloat16),
            pltpu.VMEM((n, 2, rank_here, cols), wire),
            pltpu.VMEM((n, 2, rank_here, cols), wire),
            pltpu.VMEM((16 if n == 8 else 1, 2, rank_here, cols), wire),
            pltpu.VMEM((16 if n == 8 else 1, 2, rank_here, cols), wire),
            pltpu.VMEM((2, rank_here, cols), wire),
            pltpu.VMEM((2, rank_here, cols), wire),
            pltpu.VMEM((2, rank_here, cols), jnp.float32),
            pltpu.VMEM((tp, 2, LANES), jnp.float32),
        ],
        compiler_params=pltpu.CompilerParams(
            collective_id=0, has_side_effects=True, vmem_limit_bytes=36 * 1024 * 1024
        ),
    )(*(pltpu.with_memory_space_constraint(arg, pltpu.HBM) for arg in args))
    out_hbm = pl.BlockSpec(memory_space=pltpu.HBM)
    step, new_moments, copies = pl.pallas_call(
        functools.partial(finish, n, rank * cols * tp),
        out_shape=(
            jax.ShapeDtypeStruct((deep * per_row, LANES), jnp.float32),
            jax.ShapeDtypeStruct((rank_here * per_row, LANES), jnp.float32),
            jax.ShapeDtypeStruct((depth * per_row, LANES), jnp.bfloat16),
        ),
        in_specs=[vmem] * 4,
        out_specs=(out_hbm,) * 3,
        scratch_shapes=[
            pltpu.VMEM((deep * per_row, LANES), jnp.float32),
            pltpu.VMEM((depth * per_row, LANES), jnp.bfloat16),
            dma((18,)),
        ],
        compiler_params=pltpu.CompilerParams(vmem_limit_bytes=16 * 1024 * 1024),
    )(*held)
    return from_rows(step, deep), from_rows(new_moments, rank_here), from_rows(copies, depth)


def solution(mesh):
    placed = (
        P("fs", None),
        P("fs", "tp"),
        P("fs", "tp"),
        P("fs", "tp"),
        P("fs", "tp"),
        P("tp"),
        P(),
        P("fs", None, None),
        P("fs", None, "tp"),
        P("fs", None, "tp"),
    )
    return jax.shard_map(
        functools.partial(per_device, mesh.shape["fs"], mesh.shape["tp"]),
        mesh=mesh,
        in_specs=placed,
        out_specs=(P("fs", None, "tp"), P("fs", None, "tp"), P(None, None, "tp")),
        check_vma=False,
    )
```
